32 devices in a mesh: sp: 16 (over z, y, x), tp: 2 (over core).
Axes of the slice: x: 2, y: 2, z: 4, core: 2. Of those that a mesh axis runs over, the one named last changes fastest.
Arguments:
- residual_in: bfloat16 [6144, 2048], P(('sp', 'tp')), may hold values from -6 to 6
- conv_values: bfloat16 [6144, 1024], P('sp', 'tp'), may hold values from -60 to 60
- conv_gates: bfloat16 [6144, 1024], P('sp', 'tp'), may hold values from -8 to 8
- conv_kernel: float32 [31, 1024], P(None, 'tp'), may hold values from -1 to 1
- conv_bias: float32 [1024], P('tp'), may hold values from -3 to 3
- chan_gain: float32 [1024], P('tp'), may hold values from 0.1 to 1.9
- chan_shift: float32 [1024], P('tp'), may hold values from -3 to 3
- out_weight: bfloat16 [1024, 2048], replicated, may hold values from -0.1875 to 0.1875
- norm_gain: float32 [2048], replicated, may hold values from 0.1 to 1.9
- route_ids: int32 [6144, 2], P(('sp', 'tp')), may hold values from 0 to 15, all different within a row; in each aligned block of 192 rows (0 to 191, 192 to 383, ...) at most 48 rows name the same one
- route_weights: float32 [6144, 2], P(('sp', 'tp')), may hold values from 0.25 to 1.5
- expert_gate: bfloat16 [16, 2048, 2048], P('sp', None, 'tp'), may hold values from -0.125 to 0.125
- expert_up: bfloat16 [16, 2048, 2048], P('sp', None, 'tp'), may hold values from -0.125 to 0.125
- expert_down: bfloat16 [16, 2048, 2048], P('sp', 'tp'), may hold values from -0.125 to 0.125
Outputs:
- layer_out: bfloat16 [6144, 2048], P(('sp', 'tp'))
The draws below stay inside these ranges and needn't reach their ends.
Inputs may be any that keep to these rules, and one draw needn't show every extreme that they name: `route_ids`: each row names 2 different experts. Among the rows of one device (aligned blocks of 192 rows) no expert is named by more than 48 rows, a bound that some block reaches.
All inputs are finite; a program needn't handle non-finite values.
Results may differ from the reference program's by a relative error of at most 0.014.
Values may be sent and summed in bfloat16 or wider, within the bound.
A program may use at most 128 MiB of HBM per device.

```python
import math
import jax
import jax.numpy as jnp
import numpy as np
from jax import lax

D = 2048
C = 1024
FF = 2048
KW = 31
TOPK = 2
ROWS = 192
TOKENS = 6144
EXPERTS = 16
CAP = 48
N_SP = 16
N_TP = 2


def draw_conv_values(key, part):
    keys = jax.random.split(jax.random.fold_in(key, 11), 3)
    columns = jnp.exp(jax.random.uniform(keys[0], (C,), jnp.float32, 0.0, math.log(10.0)))
    rowscale = jnp.exp(jax.random.uniform(keys[1], (TOKENS, 1), jnp.float32, 0.0, math.log(4.0)))
    base = jnp.clip(jax.random.normal(keys[2], (TOKENS, C), jnp.float32), -4.0, 4.0)
    values = jnp.clip(base * columns[None, :] * rowscale * 0.4, -60.0, 60.0)
    return values.astype(jnp.bfloat16)


def level_of(own_key, shape, pieces, smallest, high):
    def one(dim, blocks):
        draws = jax.random.uniform(jax.random.fold_in(jax.random.fold_in(own_key, 6), dim), (blocks,), jnp.float32, smallest / len(pieces), high / len(pieces))
        return jnp.repeat(jnp.exp(draws), shape[dim] // blocks).reshape((-1,) + (1,) * (len(shape) - dim - 1))

    level = one(*pieces[0])
    for cut in pieces[1:]:
        level = level * one(*cut)
    return level


def shared_out(rng, own, number, rows, amount, top, bound, lean):
    order = jax.random.permutation(rng, amount)
    packed, ordinary = portions_of(amount, rows * top, bound, lean, True), portions_of(amount, rows * top, bound, lean, False)
    places = jnp.arange(amount)

    def named(sizes, turn):
        used = int((sizes > 0).sum())
        fixed = max(1, used // 4)
        shifted = fixed + (places - fixed + turn * (used - fixed)) % max(1, amount - fixed)
        return jnp.zeros((amount,), jnp.int32).at[order[jnp.where(places < fixed, places, shifted)]].set(jnp.asarray(sizes, jnp.int32))

    sizes = jnp.where(number % 4 == 0, named(packed, number // 4), named(ordinary, number - number // 4 - 1))
    mixed = jax.random.permutation(jax.random.fold_in(own, 3), amount)
    giver, sink = mixed[0:amount // 2 * 2:2], mixed[1:amount // 2 * 2:2]
    margin = jnp.minimum(sizes[giver] - 1, bound - sizes[sink]) // 2
    margin = jnp.where((giver == order[0]) | (sink == order[0]) | (sizes[sink] == 0), 0, jnp.maximum(margin, 0))
    shifted = jax.random.randint(jax.random.fold_in(own, 4), (amount // 2,), 0, 1 << 20) % (margin + 1)
    sizes = sizes.at[giver].add(-shifted).at[sink].add(shifted)
    items = jnp.searchsorted(jnp.cumsum(sizes), jnp.arange(rows * top), side="right").astype(jnp.int32)
    grid = items.reshape(top, rows).T
    grid = grid[jax.random.permutation(jax.random.fold_in(own, 1), rows)]
    turn = jax.random.randint(jax.random.fold_in(own, 2), (rows, 1), 0, top)
    return jnp.take_along_axis(grid, (jnp.arange(top)[None, :] + turn) % top, axis=1)


def portions_of(number_of, total, bound, lean, full):
    loads = [(1 << 20) // math.isqrt(grade ** lean) + 1 for grade in range(1, number_of + 1)]
    largest = bound if full else min(bound, max(-(-total // number_of), total * loads[0] // sum(loads)))
    least = 1 if total - largest >= number_of - 1 else 0
    counts, spare = [largest] + [least] * (number_of - 1), total - largest - least * (number_of - 1)
    while spare > 0:
        movable = [i for i in range(1, number_of) if counts[i] < largest] or [i for i in range(1, number_of) if counts[i] < bound]
        pool, budget = sum([loads[i] for i in movable]), spare
        for i in movable:
            more = min(bound - counts[i], max(1, budget * loads[i] // pool), spare)
            counts[i] = counts[i] + more
            spare = spare - more
    return np.array(counts)


def centred(own_key, shape, deviation, most, pieces=(), held_as=jnp.bfloat16):
    loudness = level_of(own_key, shape, pieces, -0.22, 0.18) if pieces else 1.0
    result = jax.random.normal(own_key, shape, jnp.float32) * deviation * loudness
    return jnp.minimum(jnp.maximum(result, -most), most).astype(held_as)


def setup_inputs(seed: int = 0) -> dict:
    seeds = jax.random.split(jax.random.key(seed), 15)
    residual_in = centred(seeds[0], (TOKENS, D), 1.0, 6.0, ((0, 32),))
    conv_values = draw_conv_values(jax.random.fold_in(seeds[14], 71), 0)
    conv_gates = centred(seeds[2], (TOKENS, C), 1.5, 8.0, ((0, 16), (1, 2)))
    conv_kernel = centred(seeds[3], (KW, C), KW ** -0.5, 1.0, ((1, 2),), jnp.float32)
    conv_bias = centred(seeds[4], (C,), 0.5, 3.0, ((0, 2),), jnp.float32)
    chan_gain = jnp.clip(1.0 + 0.18 * jax.random.normal(seeds[5], (C,), jnp.float32), 0.1, 1.9)
    chan_shift = centred(seeds[6], (C,), 0.5, 3.0, ((0, 2),), jnp.float32)
    out_weight = centred(seeds[7], (C, D), C ** -0.5, 0.1875)
    norm_gain = jnp.clip(1.0 + 0.18 * jax.random.normal(seeds[8], (D,), jnp.float32), 0.1, 1.9)
    route_ids_keys = jax.random.split(jax.random.fold_in(seeds[9], 1), TOKENS // ROWS)
    route_ids_turns = jax.random.permutation(jax.random.fold_in(seeds[9], 3), TOKENS // ROWS)
    route_ids = jax.vmap(lambda own, number: shared_out(jax.random.fold_in(seeds[9], 2), own, number, ROWS, EXPERTS, TOPK, CAP, 2))(route_ids_keys, route_ids_turns).reshape((TOKENS, TOPK))
    route_weights = jnp.clip(0.25 + 1.25 * jax.random.uniform(seeds[10], (TOKENS, TOPK), jnp.float32) ** level_of(seeds[10], (TOKENS, TOPK), ((0, 32),), -0.2, 0.2), 0.25, 1.5)
    expert_gate = centred(seeds[11], (EXPERTS, D, FF), D ** -0.5, 0.125, ((0, 16), (2, 2)))
    expert_up = centred(seeds[12], (EXPERTS, D, FF), D ** -0.5, 0.125, ((0, 16), (2, 2)))
    expert_down = centred(seeds[13], (EXPERTS, FF, D), FF ** -0.5, 0.125, ((0, 16), (1, 2)))
    return {"residual_in": residual_in, "conv_values": conv_values, "conv_gates": conv_gates, "conv_kernel": conv_kernel, "conv_bias": conv_bias, "chan_gain": chan_gain, "chan_shift": chan_shift, "out_weight": out_weight, "norm_gain": norm_gain, "route_ids": route_ids, "route_weights": route_weights, "expert_gate": expert_gate, "expert_up": expert_up, "expert_down": expert_down}


def reference(residual_in, conv_values, conv_gates, conv_kernel, conv_bias, chan_gain, chan_shift, out_weight, norm_gain, route_ids, route_weights, expert_gate, expert_up, expert_down):
    seq_count = residual_in.shape[0]
    gated = (conv_values.astype(jnp.float32) * jax.nn.sigmoid(conv_gates.astype(jnp.float32))).astype(jnp.bfloat16)
    padded = jnp.concatenate([jnp.zeros((KW - 1, C), jnp.float32), gated.astype(jnp.float32)], 0)
    mixed = jnp.zeros((seq_count, C), jnp.float32) + conv_bias[None, :]
    for tap_index in range(KW):
        mixed = mixed + conv_kernel[tap_index][None, :] * padded[tap_index:tap_index + seq_count]
    center = lax.optimization_barrier(jnp.mean(mixed, 1, keepdims=True))
    spread = lax.optimization_barrier(jnp.mean(mixed * mixed, 1, keepdims=True)) - center * center
    normed = (mixed - center) * lax.rsqrt(spread + 1e-06) * chan_gain[None, :] + chan_shift[None, :]
    activated = jax.nn.silu(normed).astype(jnp.bfloat16)
    projected = jnp.dot(activated, out_weight, preferred_element_type=jnp.float32)
    after_mix = (residual_in.astype(jnp.float32) + projected).astype(jnp.bfloat16)
    after_f = after_mix.astype(jnp.float32)
    normal_rows = (after_f * lax.rsqrt(lax.optimization_barrier(jnp.mean(after_f * after_f, 1, keepdims=True)) + 1e-06) * norm_gain[None, :]).astype(jnp.bfloat16)
    flat_ids = route_ids.reshape(-1)
    flat_weights = route_weights.reshape(-1)
    most_rows = N_SP * N_TP * CAP
    half_width = FF // N_TP

    def per_expert(totals, inputs):
        gate_w, up_w, down_w, expert_index = inputs
        chosen = flat_ids == expert_index
        order = jnp.argsort(jnp.where(chosen, 0, 1).astype(jnp.int32), stable=True)[:most_rows].astype(jnp.int32)
        valid = chosen[order]
        token_index = (order // TOPK).astype(jnp.int32)
        picked = normal_rows[token_index]
        gate = jnp.dot(picked, gate_w, preferred_element_type=jnp.float32)
        upper = jnp.dot(picked, up_w, preferred_element_type=jnp.float32)
        hidden = (jax.nn.silu(gate) * upper).astype(jnp.bfloat16)
        summed = jnp.zeros((most_rows, D), jnp.float32)
        for half_index in range(N_TP):
            partial_out = jnp.dot(hidden[:, half_index * half_width:(half_index + 1) * half_width], down_w[half_index * half_width:(half_index + 1) * half_width], preferred_element_type=jnp.float32)
            partial_out = lax.optimization_barrier(partial_out.astype(jnp.bfloat16))
            summed = summed + partial_out.astype(jnp.float32)
        expert_out = summed.astype(jnp.bfloat16).astype(jnp.float32)
        weight = jnp.where(valid, flat_weights[order], 0.0)
        totals = totals.at[token_index].add(weight[:, None] * expert_out)
        return (totals, None)
    totals, unused = lax.scan(per_expert, jnp.zeros((seq_count, D), jnp.float32), (expert_gate, expert_up, expert_down, jnp.arange(EXPERTS, dtype=jnp.int32)))
    return (after_f + totals).astype(jnp.bfloat16)
```

```python
import functools

import jax
import jax.numpy as jnp
from jax import lax
from jax.experimental import pallas as pl
from jax.experimental.pallas import tpu as pltpu
from jax.sharding import PartitionSpec as P

PLANES = 4
CHUNKS = 4
MESH = pl.DeviceIdType.MESH


def flipped(index, offset):
    result, bit = index, 1
    while bit <= offset:
        if offset & bit:
            result = result + bit * (1 - 2 * ((index // bit) % 2))
        bit *= 2
    return result


def experts_kernel(
    count, cap, own, picks, weights, gate_in, up_in, down_in, out,
    dense, pick, rows, part, given, hidden, ret, zout, zin, gate_w, up_w, down_w,
    disp_sent, disp_came, plane_sent, plane_came, pair_sent, pair_came, part_sent, part_came,
    back_sent, back_came, chain_sent, chain_came, loaded,
):
    me, other = lax.axis_index("sp"), 1 - lax.axis_index("tp")
    chips = count // PLANES
    half = chips * cap
    z = me // chips
    mid = ((z + 1) // 2) % 2
    low = z // 2
    sources = (z, z + 1 - 2 * (z % 2), 2 - low, 3 * (1 - low))
    flips = (0, 1, 2 + mid, 3 - mid)
    ways = (0, 1 - 2 * (z % 2), 1 - 2 * low, 1 - 2 * low)
    landings = (
        0,
        sources[1] + (PLANES - sources[1]) * (z % 2),
        sources[2] + (PLANES - sources[2]) * low * (1 - z % 2),
        sources[3],
    )
    is_mid, is_end = mid == 1, mid == 0
    has_left, has_right = z > 0, z < PLANES - 1
    wide = own.shape[1] // CHUNKS

    def cols(number):
        return pl.ds(pl.multiple_of(number * wide, wide), wide)

    def along(way):
        return {"sp": me + way * chips}

    def dispatch(turn, way, slot):
        return pltpu.make_async_remote_copy(
            src_ref=own if turn == 0 else dense.at[sources[turn]],
            dst_ref=dense.at[sources[turn]],
            send_sem=disp_sent.at[turn, slot],
            recv_sem=disp_came.at[sources[turn]],
            device_id=along(way),
            device_id_type=MESH,
        )

    def plane_copy(turn, place):
        return pltpu.make_async_remote_copy(
            src_ref=pick.at[turn, pl.ds(place * cap, cap)],
            dst_ref=rows.at[turn, pl.ds(place * cap, cap)],
            send_sem=plane_sent.at[turn, place],
            recv_sem=plane_came.at[turn, place],
            device_id={"sp": flipped(me, place)},
            device_id_type=MESH,
        )

    def pair_copy(turn):
        return pltpu.make_async_remote_copy(
            src_ref=rows.at[turn, pl.ds(0, half)],
            dst_ref=rows.at[turn, pl.ds(half, half)],
            send_sem=pair_sent.at[turn],
            recv_sem=pair_came.at[turn],
            device_id={"tp": other},
            device_id_type=MESH,
        )

    def share_copy(turn, number):
        return pltpu.make_async_remote_copy(
            src_ref=part.at[turn, pl.ds(half, half), cols(number)],
            dst_ref=given.at[turn, :, cols(number)],
            send_sem=part_sent.at[turn, number],
            recv_sem=part_came.at[turn, number],
            device_id={"tp": other},
            device_id_type=MESH,
        )

    def back_copy(turn, number, place):
        return pltpu.make_async_remote_copy(
            src_ref=part.at[turn, pl.ds(place * cap, cap), cols(number)],
            dst_ref=ret.at[turn, pl.ds(place * cap, cap), cols(number)],
            send_sem=back_sent.at[turn, number, place],
            recv_sem=back_came.at[turn, number, place],
            device_id={"sp": flipped(me, place)},
            device_id_type=MESH,
        )

    def chain_copy(turn, number, landing=None):
        landing = landings[turn] if landing is None else landing
        return pltpu.make_async_remote_copy(
            src_ref=zout.at[turn, :, cols(number)],
            dst_ref=zin.at[landing, :, cols(number)],
            send_sem=chain_sent.at[turn, number],
            recv_sem=chain_came.at[landing, number],
            device_id=along(ways[turn]),
            device_id_type=MESH,
        )

    loads = [
        pltpu.make_async_copy(source.at[0], target, loaded.at[number])
        for number, (source, target) in enumerate(
            ((gate_in, gate_w), (up_in, up_w), (down_in, down_w))
        )
    ]
    for load in loads:
        load.start()

    barrier = pltpu.get_barrier_semaphore()
    for place in range(1, chips):
        pl.semaphore_signal(
            barrier, inc=1, device_id={"sp": flipped(me, place)}, device_id_type=MESH
        )
    pl.semaphore_signal(barrier, inc=1, device_id={"tp": other}, device_id_type=MESH)

    @pl.when(has_left)
    def _():
        pl.semaphore_signal(barrier, inc=1, device_id=along(-1), device_id_type=MESH)

    @pl.when(has_right)
    def _():
        pl.semaphore_signal(barrier, inc=1, device_id=along(1), device_id_type=MESH)

    pl.semaphore_wait(barrier, chips + (z + 2) // 3 + (PLANES + 1 - z) // 3)

    def send_own(way, slot):
        dispatch(0, way, slot).start()

    pl.when(has_left)(lambda: send_own(-1, 0))
    pl.when(has_right)(lambda: send_own(1, 1))

    def select(turn):
        block = own if turn == 0 else dense.at[sources[turn]]

        def step(number, carry):
            chosen = jnp.dot(
                picks[flips[turn]], block[:, cols(number)], preferred_element_type=jnp.float32
            ).astype(jnp.bfloat16)
            rows[turn, pl.ds(0, cap), cols(number)] = chosen[:cap]
            pick[turn, :, cols(number)] = chosen
            return carry

        lax.fori_loop(0, CHUNKS, step, 0)
        for place in range(1, chips):
            plane_copy(turn, place).start()

    def arrive(turn, forward):
        dispatch(turn, 0, 0).wait_recv()
        if forward:
            dispatch(turn, -ways[turn], 0).start()

    def expert(turn):
        for place in range(1, chips):
            plane_copy(turn, place).wait_recv()
        pair_copy(turn).start()
        if turn == 0:
            for load in loads:
                load.wait()
        pair_copy(turn).wait_recv()
        narrow = min(256, gate_w.shape[1])

        def first(step, carry):
            columns = pl.ds(pl.multiple_of(step * narrow, narrow), narrow)
            gate = jnp.dot(rows[turn], gate_w[:, columns], preferred_element_type=jnp.float32)
            upper = jnp.dot(rows[turn], up_w[:, columns], preferred_element_type=jnp.float32)
            hidden[:, columns] = (jax.nn.silu(gate) * upper).astype(jnp.bfloat16)
            return carry

        lax.fori_loop(0, gate_w.shape[1] // narrow, first, 0)

        def second(number, carry):
            part[turn, :, cols(number)] = jnp.dot(
                hidden[...], down_w[:, cols(number)], preferred_element_type=jnp.float32
            ).astype(jnp.bfloat16)
            share_copy(turn, number).start()
            return carry

        lax.fori_loop(0, CHUNKS, second, 0)

        def third(number, carry):
            share_copy(turn, number).wait_recv()
            total = (
                part[turn, pl.ds(0, half), cols(number)].astype(jnp.float32)
                + given[turn, :, cols(number)].astype(jnp.float32)
            ).astype(jnp.bfloat16)
            part[turn, pl.ds(0, half), cols(number)] = total
            ret[turn, pl.ds(0, cap), cols(number)] = total[:cap]
            for place in range(1, chips):
                back_copy(turn, number, place).start()
            return carry

        lax.fori_loop(0, CHUNKS, third, 0)

    def combined(turn, number):
        for place in range(1, chips):
            back_copy(turn, number, place).wait_recv()
        block = ret[turn, :, cols(number)]
        return jnp.dot(
            weights[flips[turn], 0], block, preferred_element_type=jnp.float32
        ) + jnp.dot(weights[flips[turn], 1], block, preferred_element_type=jnp.float32)

    def end_chain(turn):
        def step(number, carry):
            zout[turn, :, cols(number)] = combined(turn, number).astype(jnp.bfloat16)
            chain_copy(turn, number).start()
            return carry

        lax.fori_loop(0, CHUNKS, step, 0)

    def mid_link(turn, number):
        partial = combined(turn, number)
        chain_copy(turn, number, sources[turn]).wait_recv()
        zout[turn, :, cols(number)] = (
            partial + zin[sources[turn], :, cols(number)].astype(jnp.float32)
        ).astype(jnp.bfloat16)
        chain_copy(turn, number).start()

    select(0)
    expert(0)

    @pl.when(is_mid)
    def _():
        arrive(1, True)
        arrive(2, True)
        select(1)
        select(2)

    @pl.when(is_end)
    def _():
        arrive(1, False)
        select(1)

    expert(1)

    @pl.when(is_mid)
    def _():
        arrive(3, True)
        select(3)

    @pl.when(is_end)
    def _():
        arrive(2, False)
        select(2)
        end_chain(1)

    expert(2)

    @pl.when(is_end)
    def _():
        arrive(3, False)
        select(3)
        end_chain(2)

    expert(3)

    @pl.when(is_end)
    def _():
        end_chain(3)

    @pl.when(is_mid)
    def _():
        for number in range(CHUNKS):
            mid_link(2, number)
        mid_link(3, 0)
        for number in range(1, CHUNKS):
            mid_link(3, number)
            mid_link(1, number - 1)
        mid_link(1, CHUNKS - 1)

    def finish(number, carry):
        out[:, cols(number)] = combined(0, number)

        def joined(landing):
            chain_copy(1, number, landing).wait_recv()
            out[:, cols(number)] += zin[landing, :, cols(number)].astype(jnp.float32)

        pl.when(has_left)(lambda: joined(z))
        pl.when(has_right)(lambda: joined(PLANES))
        return carry

    lax.fori_loop(0, CHUNKS, finish, 0)

    pl.when(has_left)(lambda: dispatch(0, -1, 0).wait_send())
    pl.when(has_right)(lambda: dispatch(0, 1, 1).wait_send())

    @pl.when(is_mid)
    def _():
        for turn in range(1, PLANES):
            dispatch(turn, -ways[turn], 0).wait_send()

    for turn in range(PLANES):
        pair_copy(turn).wait_send()
        for place in range(1, chips):
            plane_copy(turn, place).wait_send()

        def drain(number, carry, turn=turn):
            share_copy(turn, number).wait_send()
            for place in range(1, chips):
                back_copy(turn, number, place).wait_send()
            if turn:
                chain_copy(turn, number).wait_send()
            return carry

        lax.fori_loop(0, CHUNKS, drain, 0)


def run_experts(own, picks, weights, expert_gate, expert_up, expert_down, count, cap):
    row_count, width = own.shape
    units = expert_gate.shape[2]
    chips = count // PLANES
    half = chips * cap
    dma = lambda *shape: pltpu.SemaphoreType.DMA(shape)
    vmem = pl.BlockSpec(memory_space=pltpu.VMEM)
    anywhere = pl.BlockSpec(memory_space=pl.ANY)
    held = jnp.bfloat16
    return pl.pallas_call(
        functools.partial(experts_kernel, count, cap),
        out_shape=jax.ShapeDtypeStruct((row_count, width), jnp.float32),
        in_specs=[vmem, vmem, vmem, anywhere, anywhere, anywhere],
        out_specs=vmem,
        scratch_shapes=[
            pltpu.VMEM((PLANES, row_count, width), held),
            pltpu.VMEM((PLANES, half, width), held),
            pltpu.VMEM((PLANES, 2 * half, width), held),
            pltpu.VMEM((PLANES, 2 * half, width), held),
            pltpu.VMEM((PLANES, half, width), held),
            pltpu.VMEM((2 * half, units), held),
            pltpu.VMEM((PLANES, half, width), held),
            pltpu.VMEM((PLANES, row_count, width), held),
            pltpu.VMEM((PLANES + 1, row_count, width), held),
            pltpu.VMEM((width, units), held),
            pltpu.VMEM((width, units), held),
            pltpu.VMEM((units, width), held),
            dma(PLANES, 2), dma(PLANES),
            dma(PLANES, chips), dma(PLANES, chips),
            dma(PLANES), dma(PLANES),
            dma(PLANES, CHUNKS), dma(PLANES, CHUNKS),
            dma(PLANES, CHUNKS, chips), dma(PLANES, CHUNKS, chips),
            dma(PLANES, CHUNKS), dma(PLANES + 1, CHUNKS),
            dma(3),
        ],
        compiler_params=pltpu.CompilerParams(
            collective_id=0, has_side_effects=True, vmem_limit_bytes=62 * 1024 * 1024
        ),
    )(own, picks, weights, expert_gate, expert_up, expert_down)


def from_behind(value, axis, steps):
    count = lax.axis_size(axis)
    first, last = (max(0, -steps), min(count, count - steps))
    return lax.ppermute(value, axis, [(source, source + steps) for source in range(first, last)])


def swap(value, axis, offset):
    count = lax.axis_size(axis)
    return lax.ppermute(value, axis, [(source, source ^ offset) for source in range(count)])


def on_device(
    residual_in,
    conv_values,
    conv_gates,
    conv_kernel,
    conv_bias,
    chan_gain,
    chan_shift,
    out_weight,
    norm_gain,
    route_ids,
    route_weights,
    expert_gate,
    expert_up,
    expert_down,
):
    taps_count = conv_kernel.shape[0]
    tok_count, local_chan = conv_values.shape
    tp_count = lax.axis_size("tp")
    all_chan = local_chan * tp_count
    core = lax.axis_index("tp")
    gated = (
        conv_values.astype(jnp.float32) * jax.nn.sigmoid(conv_gates.astype(jnp.float32))
    ).astype(jnp.bfloat16)
    earlier = from_behind(gated[tok_count - (taps_count - 1) :], "sp", 1)
    extended = jnp.concatenate([earlier, gated], 0).astype(jnp.float32)
    mixed = jnp.zeros((tok_count, local_chan), jnp.float32) + conv_bias[None, :]
    for tap_index in range(taps_count):
        mixed = (
            mixed + conv_kernel[tap_index][None, :] * extended[tap_index : tap_index + tok_count]
        )
    sums = jnp.stack([jnp.sum(mixed, 1), jnp.sum(mixed * mixed, 1)])
    sums = sums + swap(sums, "tp", 1)
    center = (sums[0] / all_chan)[:, None]
    spread = (sums[1] / all_chan)[:, None] - center * center
    normed = (mixed - center) * lax.rsqrt(spread + 1e-06) * chan_gain[None, :] + chan_shift[None, :]
    activated = jax.nn.silu(normed).astype(jnp.bfloat16)
    row_count = tok_count // tp_count
    low, high = activated[:row_count], activated[row_count:]
    kept = jnp.where(core == 0, low, high)
    given = swap(jnp.where(core == 0, high, low), "tp", 1)
    regrouped = jnp.concatenate(
        [jnp.where(core == 0, kept, given), jnp.where(core == 0, given, kept)], 1
    )
    projected = jnp.dot(regrouped, out_weight, preferred_element_type=jnp.float32)
    after_f = (residual_in.astype(jnp.float32) + projected).astype(jnp.bfloat16).astype(jnp.float32)
    normal_rows = (
        after_f
        * lax.rsqrt(jnp.mean(after_f * after_f, 1, keepdims=True) + 1e-06)
        * norm_gain[None, :]
    ).astype(jnp.bfloat16)
    sp_count = lax.axis_size("sp")
    experts_all = expert_gate.shape[0] * sp_count
    choose_count = route_ids.shape[1]
    slot_cap = max(2, (2 * choose_count * row_count + experts_all - 1) // experts_all)
    slot_cap = (slot_cap + 15) // 16 * 16
    onehot = (
        route_ids.reshape(-1)[:, None] == jnp.arange(experts_all, dtype=jnp.int32)[None, :]
    ).astype(jnp.int32)
    before = jnp.cumsum(onehot, 0) - onehot
    ranking = jnp.sum(before * onehot, 1).reshape(row_count, choose_count)
    chips = sp_count // PLANES
    half = chips * slot_cap
    me = lax.axis_index("sp")
    plane, place = me // chips, me % chips
    target_plane, target_place = route_ids // chips, route_ids % chips
    slot_ids = target_plane * half + (target_place ^ place) * slot_cap + ranking
    routing = jnp.concatenate([slot_ids.astype(jnp.float32), route_weights], 1).T
    routings = [routing] + [swap(routing, "sp", flip * chips) for flip in range(1, PLANES)]
    base = (plane * half).astype(jnp.float32)
    slots = lax.broadcasted_iota(jnp.int32, (half, 1), 0).astype(jnp.float32) + base
    lanes = lax.broadcasted_iota(jnp.int32, (1, half), 1).astype(jnp.float32) + base
    picks, weights = [], []
    for held in routings:
        ids, scales = held[:choose_count], held[choose_count:]
        chosen = functools.reduce(
            jnp.logical_or, [slots == ids[choice][None, :] for choice in range(choose_count)]
        )
        picks.append(chosen.astype(jnp.bfloat16))
        weighting = sum(
            jnp.where(lanes == ids[choice][:, None], scales[choice][:, None], 0.0)
            for choice in range(choose_count)
        )
        coarse_f = lax.reduce_precision(weighting, 8, 7)
        weights.append(
            jnp.stack([coarse_f.astype(jnp.bfloat16), (weighting - coarse_f).astype(jnp.bfloat16)])
        )
    summed = run_experts(
        normal_rows, jnp.stack(picks), jnp.stack(weights),
        expert_gate, expert_up, expert_down, sp_count, slot_cap,
    )
    combined = after_f + summed
    return combined.astype(jnp.bfloat16)


def solution(mesh):
    placed = (
        P(("sp", "tp"), None),
        P("sp", "tp"),
        P("sp", "tp"),
        P(None, "tp"),
        P("tp"),
        P("tp"),
        P("tp"),
        P(),
        P(),
        P(("sp", "tp"), None),
        P(("sp", "tp"), None),
        P("sp", None, "tp"),
        P("sp", None, "tp"),
        P("sp", "tp", None),
    )
    return jax.shard_map(
        on_device, mesh=mesh, in_specs=placed, out_specs=P(("sp", "tp"), None), check_vma=False
    )
```

```python
import functools

import jax
import jax.numpy as jnp
from jax import lax
from jax.experimental import pallas as pl
from jax.experimental.pallas import tpu as pltpu
from jax.sharding import PartitionSpec as P

PLANES = 4
CHUNKS = 4
MESH = pl.DeviceIdType.MESH


def flipped(index, offset):
    result, bit = index, 1
    while bit <= offset:
        if offset & bit:
            result = result + bit * (1 - 2 * ((index // bit) % 2))
        bit *= 2
    return result


def experts_kernel(
    count, cap, own, picks, weights, gate_in, up_in, down_in, out,
    dense, pick, rows, part, given, hidden, ret, zout, zin, gate_w, up_w, down_w,
    disp_sent, disp_came, plane_sent, plane_came, pair_sent, pair_came, part_sent, part_came,
    back_sent, back_came, chain_sent, chain_came, loaded,
):
    me, other = lax.axis_index("sp"), 1 - lax.axis_index("tp")
    chips = count // PLANES
    half = chips * cap
    z = me // chips
    mid = ((z + 1) // 2) % 2
    low = z // 2
    sources = (z, z + 1 - 2 * (z % 2), 2 - low, 3 * (1 - low))
    flips = (0, 1, 2 + mid, 3 - mid)
    ways = (0, 1 - 2 * (z % 2), 1 - 2 * low, 1 - 2 * low)
    landings = (
        0,
        sources[1] + (PLANES - sources[1]) * (z % 2),
        sources[2] + (PLANES - sources[2]) * low * (1 - z % 2),
        sources[3],
    )
    is_mid, is_end = mid == 1, mid == 0
    has_left, has_right = z > 0, z < PLANES - 1
    wide = own.shape[1] // CHUNKS

    def cols(number):
        return pl.ds(pl.multiple_of(number * wide, wide), wide)

    def along(way):
        return {"sp": me + way * chips}

    def dispatch(turn, number, way, slot):
        block = own if turn == 0 else dense.at[sources[turn]]
        return pltpu.make_async_remote_copy(
            src_ref=block.at[:, cols(number)],
            dst_ref=dense.at[sources[turn], :, cols(number)],
            send_sem=disp_sent.at[turn, number, slot],
            recv_sem=disp_came.at[sources[turn], number],
            device_id=along(way),
            device_id_type=MESH,
        )

    def plane_copy(turn, number, place):
        return pltpu.make_async_remote_copy(
            src_ref=pick.at[turn, pl.ds(place * cap, cap), cols(number)],
            dst_ref=rows.at[turn, pl.ds(place * cap, cap), cols(number)],
            send_sem=plane_sent.at[turn, number, place],
            recv_sem=plane_came.at[turn, number, place],
            device_id={"sp": flipped(me, place)},
            device_id_type=MESH,
        )

    def pair_copy(turn, number):
        return pltpu.make_async_remote_copy(
            src_ref=rows.at[turn, pl.ds(0, half), cols(number)],
            dst_ref=rows.at[turn, pl.ds(half, half), cols(number)],
            send_sem=pair_sent.at[turn, number],
            recv_sem=pair_came.at[turn, number],
            device_id={"tp": other},
            device_id_type=MESH,
        )

    def share_copy(turn, number):
        return pltpu.make_async_remote_copy(
            src_ref=part.at[turn, pl.ds(half, half), cols(number)],
            dst_ref=given.at[turn, :, cols(number)],
            send_sem=part_sent.at[turn, number],
            recv_sem=part_came.at[turn, number],
            device_id={"tp": other},
            device_id_type=MESH,
        )

    def back_copy(turn, number, place):
        return pltpu.make_async_remote_copy(
            src_ref=part.at[turn, pl.ds(place * cap, cap), cols(number)],
            dst_ref=ret.at[turn, pl.ds(place * cap, cap), cols(number)],
            send_sem=back_sent.at[turn, number, place],
            recv_sem=back_came.at[turn, number, place],
            device_id={"sp": flipped(me, place)},
            device_id_type=MESH,
        )

    def chain_copy(turn, number, landing=None):
        landing = landings[turn] if landing is None else landing
        return pltpu.make_async_remote_copy(
            src_ref=zout.at[turn, :, cols(number)],
            dst_ref=zin.at[landing, :, cols(number)],
            send_sem=chain_sent.at[turn, number],
            recv_sem=chain_came.at[landing, number],
            device_id=along(ways[turn]),
            device_id_type=MESH,
        )

    loads = [
        pltpu.make_async_copy(source.at[0], target, loaded.at[number])
        for number, (source, target) in enumerate(
            ((gate_in, gate_w), (up_in, up_w), (down_in, down_w))
        )
    ]
    for load in loads:
        load.start()

    barrier = pltpu.get_barrier_semaphore()
    for place in range(1, chips):
        pl.semaphore_signal(
            barrier, inc=1, device_id={"sp": flipped(me, place)}, device_id_type=MESH
        )
    pl.semaphore_signal(barrier, inc=1, device_id={"tp": other}, device_id_type=MESH)

    @pl.when(has_left)
    def _():
        pl.semaphore_signal(barrier, inc=1, device_id=along(-1), device_id_type=MESH)

    @pl.when(has_right)
    def _():
        pl.semaphore_signal(barrier, inc=1, device_id=along(1), device_id_type=MESH)

    pl.semaphore_wait(barrier, chips + (z + 2) // 3 + (PLANES + 1 - z) // 3)

    def send_own(number, carry):
        pl.when(has_left)(lambda: dispatch(0, number, -1, 0).start())
        pl.when(has_right)(lambda: dispatch(0, number, 1, 1).start())
        return carry

    lax.fori_loop(0, CHUNKS, send_own, 0)

    def select(turn, number):
        block = own if turn == 0 else dense.at[sources[turn]]
        chosen = jnp.dot(
            picks[flips[turn]], block[:, cols(number)], preferred_element_type=jnp.float32
        ).astype(jnp.bfloat16)
        rows[turn, pl.ds(0, cap), cols(number)] = chosen[:cap]
        pick[turn, :, cols(number)] = chosen
        for place in range(1, chips):
            plane_copy(turn, number, place).start()

    def arrive(turn, number, forward):
        dispatch(turn, number, 0, 0).wait_recv()
        if forward:
            dispatch(turn, number, -ways[turn], 0).start()
        select(turn, number)

    def gather(turn):
        def step(number, carry):
            for place in range(1, chips):
                plane_copy(turn, number, place).wait_recv()
            pair_copy(turn, number).start()
            return carry

        lax.fori_loop(0, CHUNKS, step, 0)
        if turn == 0:
            for load in loads:
                load.wait()

        def joined(number, carry):
            pair_copy(turn, number).wait_recv()
            return carry

        lax.fori_loop(0, CHUNKS, joined, 0)

    def first(turn):
        narrow = min(256, gate_w.shape[1])

        def step(number, carry):
            columns = pl.ds(pl.multiple_of(number * narrow, narrow), narrow)
            gate = jnp.dot(rows[turn], gate_w[:, columns], preferred_element_type=jnp.float32)
            upper = jnp.dot(rows[turn], up_w[:, columns], preferred_element_type=jnp.float32)
            hidden[:, columns] = (jax.nn.silu(gate) * upper).astype(jnp.bfloat16)
            return carry

        lax.fori_loop(0, gate_w.shape[1] // narrow, step, 0)

    def second(turn):
        def step(number, carry):
            part[turn, :, cols(number)] = jnp.dot(
                hidden[...], down_w[:, cols(number)], preferred_element_type=jnp.float32
            ).astype(jnp.bfloat16)
            share_copy(turn, number).start()
            return carry

        lax.fori_loop(0, CHUNKS, step, 0)

    def third(turn):
        def step(number, carry):
            share_copy(turn, number).wait_recv()
            total = (
                part[turn, pl.ds(0, half), cols(number)].astype(jnp.float32)
                + given[turn, :, cols(number)].astype(jnp.float32)
            ).astype(jnp.bfloat16)
            part[turn, pl.ds(0, half), cols(number)] = total
            ret[turn, pl.ds(0, cap), cols(number)] = total[:cap]
            for place in range(1, chips):
                back_copy(turn, number, place).start()
            return carry

        lax.fori_loop(0, CHUNKS, step, 0)

    def combined(turn, number):
        for place in range(1, chips):
            back_copy(turn, number, place).wait_recv()
        block = ret[turn, :, cols(number)]
        return jnp.dot(
            weights[flips[turn], 0], block, preferred_element_type=jnp.float32
        ) + jnp.dot(weights[flips[turn], 1], block, preferred_element_type=jnp.float32)

    def end_chain(turn):
        def step(number, carry):
            zout[turn, :, cols(number)] = combined(turn, number).astype(jnp.bfloat16)
            chain_copy(turn, number).start()
            return carry

        lax.fori_loop(0, CHUNKS, step, 0)

    def mid_link(turn, number):
        partial = combined(turn, number)
        chain_copy(turn, number, sources[turn]).wait_recv()
        zout[turn, :, cols(number)] = (
            partial + zin[sources[turn], :, cols(number)].astype(jnp.float32)
        ).astype(jnp.bfloat16)
        chain_copy(turn, number).start()

    def at_mid(turn, begin, end):
        @pl.when(is_mid)
        def _():
            for number in range(begin, end):
                arrive(turn, number, True)

    def at_end(turn, begin, end):
        @pl.when(is_end)
        def _():
            for number in range(begin, end):
                arrive(turn, number, False)

    def near(begin, end):
        for number in range(begin, end):
            at_mid(1, number, number + 1)
            at_mid(2, number, number + 1)
            at_end(1, number, number + 1)

    for number in range(CHUNKS):
        select(0, number)
    near(0, CHUNKS // 2)
    gather(0)
    first(0)
    near(CHUNKS // 2, CHUNKS)
    second(0)
    at_mid(3, 0, CHUNKS // 4)
    at_end(2, 0, CHUNKS // 4)
    gather(1)
    first(1)
    at_mid(3, CHUNKS // 4, CHUNKS // 2)
    at_end(2, CHUNKS // 4, CHUNKS // 2)
    second(1)
    third(1)
    at_mid(3, CHUNKS // 2, CHUNKS)
    at_end(2, CHUNKS // 2, CHUNKS)
    pl.when(is_end)(lambda: end_chain(1))
    at_end(3, 0, CHUNKS // 4)
    gather(2)
    first(2)
    at_end(3, CHUNKS // 4, CHUNKS // 2)
    second(2)
    third(2)
    at_end(3, CHUNKS // 2, CHUNKS)
    pl.when(is_end)(lambda: end_chain(2))
    third(0)
    gather(3)
    first(3)
    second(3)
    third(3)
    pl.when(is_end)(lambda: end_chain(3))

    @pl.when(is_mid)
    def _():
        for number in range(CHUNKS):
            mid_link(2, number)
        mid_link(3, 0)
        for number in range(1, CHUNKS):
            mid_link(3, number)
            mid_link(1, number - 1)
        mid_link(1, CHUNKS - 1)

    def finish(number, carry):
        out[:, cols(number)] = combined(0, number)

        def joined(landing):
            chain_copy(1, number, landing).wait_recv()
            out[:, cols(number)] += zin[landing, :, cols(number)].astype(jnp.float32)

        pl.when(has_left)(lambda: joined(z))
        pl.when(has_right)(lambda: joined(PLANES))
        return carry

    lax.fori_loop(0, CHUNKS, finish, 0)

    def drain(number, carry):
        pl.when(has_left)(lambda: dispatch(0, number, -1, 0).wait_send())
        pl.when(has_right)(lambda: dispatch(0, number, 1, 1).wait_send())

        @pl.when(is_mid)
        def _():
            for turn in range(1, PLANES):
                dispatch(turn, number, -ways[turn], 0).wait_send()

        for turn in range(PLANES):
            pair_copy(turn, number).wait_send()
            share_copy(turn, number).wait_send()
            for place in range(1, chips):
                plane_copy(turn, number, place).wait_send()
                back_copy(turn, number, place).wait_send()
            if turn:
                chain_copy(turn, number).wait_send()
        return carry

    lax.fori_loop(0, CHUNKS, drain, 0)


def run_experts(own, picks, weights, expert_gate, expert_up, expert_down, count, cap):
    row_count, width = own.shape
    units = expert_gate.shape[2]
    chips = count // PLANES
    half = chips * cap
    dma = lambda *shape: pltpu.SemaphoreType.DMA(shape)
    vmem = pl.BlockSpec(memory_space=pltpu.VMEM)
    anywhere = pl.BlockSpec(memory_space=pl.ANY)
    held = jnp.bfloat16
    return pl.pallas_call(
        functools.partial(experts_kernel, count, cap),
        out_shape=jax.ShapeDtypeStruct((row_count, width), jnp.float32),
        in_specs=[vmem, vmem, vmem, anywhere, anywhere, anywhere],
        out_specs=vmem,
        scratch_shapes=[
            pltpu.VMEM((PLANES, row_count, width), held),
            pltpu.VMEM((PLANES, half, width), held),
            pltpu.VMEM((PLANES, 2 * half, width), held),
            pltpu.VMEM((PLANES, 2 * half, width), held),
            pltpu.VMEM((PLANES, half, width), held),
            pltpu.VMEM((2 * half, units), held),
            pltpu.VMEM((PLANES, half, width), held),
            pltpu.VMEM((PLANES, row_count, width), held),
            pltpu.VMEM((PLANES + 1, row_count, width), held),
            pltpu.VMEM((width, units), held),
            pltpu.VMEM((width, units), held),
            pltpu.VMEM((units, width), held),
            dma(PLANES, CHUNKS, 2), dma(PLANES, CHUNKS),
            dma(PLANES, CHUNKS, chips), dma(PLANES, CHUNKS, chips),
            dma(PLANES, CHUNKS), dma(PLANES, CHUNKS),
            dma(PLANES, CHUNKS), dma(PLANES, CHUNKS),
            dma(PLANES, CHUNKS, chips), dma(PLANES, CHUNKS, chips),
            dma(PLANES, CHUNKS), dma(PLANES + 1, CHUNKS),
            dma(3),
        ],
        compiler_params=pltpu.CompilerParams(
            collective_id=0, has_side_effects=True, vmem_limit_bytes=62 * 1024 * 1024
        ),
    )(own, picks, weights, expert_gate, expert_up, expert_down)


def from_behind(value, axis, steps):
    count = lax.axis_size(axis)
    first, last = (max(0, -steps), min(count, count - steps))
    return lax.ppermute(value, axis, [(source, source + steps) for source in range(first, last)])


def swap(value, axis, offset):
    count = lax.axis_size(axis)
    return lax.ppermute(value, axis, [(source, source ^ offset) for source in range(count)])


def on_device(
    residual_in,
    conv_values,
    conv_gates,
    conv_kernel,
    conv_bias,
    chan_gain,
    chan_shift,
    out_weight,
    norm_gain,
    route_ids,
    route_weights,
    expert_gate,
    expert_up,
    expert_down,
):
    taps_count = conv_kernel.shape[0]
    tok_count, local_chan = conv_values.shape
    tp_count = lax.axis_size("tp")
    all_chan = local_chan * tp_count
    core = lax.axis_index("tp")
    gated = (
        conv_values.astype(jnp.float32) * jax.nn.sigmoid(conv_gates.astype(jnp.float32))
    ).astype(jnp.bfloat16)
    earlier = from_behind(gated[tok_count - (taps_count - 1) :], "sp", 1)
    extended = jnp.concatenate([earlier, gated], 0).astype(jnp.float32)
    mixed = jnp.zeros((tok_count, local_chan), jnp.float32) + conv_bias[None, :]
    for tap_index in range(taps_count):
        mixed = (
            mixed + conv_kernel[tap_index][None, :] * extended[tap_index : tap_index + tok_count]
        )
    sums = jnp.stack([jnp.sum(mixed, 1), jnp.sum(mixed * mixed, 1)])
    sums = sums + swap(sums, "tp", 1)
    center = (sums[0] / all_chan)[:, None]
    spread = (sums[1] / all_chan)[:, None] - center * center
    normed = (mixed - center) * lax.rsqrt(spread + 1e-06) * chan_gain[None, :] + chan_shift[None, :]
    activated = jax.nn.silu(normed).astype(jnp.bfloat16)
    row_count = tok_count // tp_count
    low, high = activated[:row_count], activated[row_count:]
    kept = jnp.where(core == 0, low, high)
    given = swap(jnp.where(core == 0, high, low), "tp", 1)
    regrouped = jnp.concatenate(
        [jnp.where(core == 0, kept, given), jnp.where(core == 0, given, kept)], 1
    )
    projected = jnp.dot(regrouped, out_weight, preferred_element_type=jnp.float32)
    after_f = (residual_in.astype(jnp.float32) + projected).astype(jnp.bfloat16).astype(jnp.float32)
    normal_rows = (
        after_f
        * lax.rsqrt(jnp.mean(after_f * after_f, 1, keepdims=True) + 1e-06)
        * norm_gain[None, :]
    ).astype(jnp.bfloat16)
    sp_count = lax.axis_size("sp")
    experts_all = expert_gate.shape[0] * sp_count
    choose_count = route_ids.shape[1]
    slot_cap = max(2, (2 * choose_count * row_count + experts_all - 1) // experts_all)
    slot_cap = (slot_cap + 15) // 16 * 16
    onehot = (
        route_ids.reshape(-1)[:, None] == jnp.arange(experts_all, dtype=jnp.int32)[None, :]
    ).astype(jnp.int32)
    before = jnp.cumsum(onehot, 0) - onehot
    ranking = jnp.sum(before * onehot, 1).reshape(row_count, choose_count)
    chips = sp_count // PLANES
    half = chips * slot_cap
    me = lax.axis_index("sp")
    plane, place = me // chips, me % chips
    target_plane, target_place = route_ids // chips, route_ids % chips
    slot_ids = target_plane * half + (target_place ^ place) * slot_cap + ranking
    routing = jnp.concatenate([slot_ids.astype(jnp.float32), route_weights], 1).T
    routings = [routing] + [swap(routing, "sp", flip * chips) for flip in range(1, PLANES)]
    base = (plane * half).astype(jnp.float32)
    slots = lax.broadcasted_iota(jnp.int32, (half, 1), 0).astype(jnp.float32) + base
    lanes = lax.broadcasted_iota(jnp.int32, (1, half), 1).astype(jnp.float32) + base
    picks, weights = [], []
    for held in routings:
        ids, scales = held[:choose_count], held[choose_count:]
        chosen = functools.reduce(
            jnp.logical_or, [slots == ids[choice][None, :] for choice in range(choose_count)]
        )
        picks.append(chosen.astype(jnp.bfloat16))
        weighting = sum(
            jnp.where(lanes == ids[choice][:, None], scales[choice][:, None], 0.0)
            for choice in range(choose_count)
        )
        coarse_f = lax.reduce_precision(weighting, 8, 7)
        weights.append(
            jnp.stack([coarse_f.astype(jnp.bfloat16), (weighting - coarse_f).astype(jnp.bfloat16)])
        )
    summed = run_experts(
        normal_rows, jnp.stack(picks), jnp.stack(weights),
        expert_gate, expert_up, expert_down, sp_count, slot_cap,
    )
    combined = after_f + summed
    return combined.astype(jnp.bfloat16)


def solution(mesh):
    placed = (
        P(("sp", "tp"), None),
        P("sp", "tp"),
        P("sp", "tp"),
        P(None, "tp"),
        P("tp"),
        P("tp"),
        P("tp"),
        P(),
        P(),
        P(("sp", "tp"), None),
        P(("sp", "tp"), None),
        P("sp", None, "tp"),
        P("sp", None, "tp"),
        P("sp", "tp", None),
    )
    return jax.shard_map(
        on_device, mesh=mesh, in_specs=placed, out_specs=P(("sp", "tp"), None), check_vma=False
    )
```

```python
import functools

import jax
import jax.numpy as jnp
from jax import lax
from jax.experimental import pallas as pl
from jax.experimental.pallas import tpu as pltpu
from jax.sharding import PartitionSpec as P

PLANES = 4
CHUNKS = 8
MESH = pl.DeviceIdType.MESH


def flipped(index, offset):
    result, bit = index, 1
    while bit <= offset:
        if offset & bit:
            result = result + bit * (1 - 2 * ((index // bit) % 2))
        bit *= 2
    return result


def experts_kernel(
    count, cap, own, picks, weights, gate_in, up_in, down_in, out,
    dense, pick, rows, part, given, hidden, ret, zout, zin, gate_w, up_w, down_w,
    disp_sent, disp_came, plane_sent, plane_came, pair_sent, pair_came, part_sent, part_came,
    back_sent, back_came, chain_sent, chain_came, loaded,
):
    me, other = lax.axis_index("sp"), 1 - lax.axis_index("tp")
    chips = count // PLANES
    half = chips * cap
    z = me // chips
    mid = ((z + 1) // 2) % 2
    low = z // 2
    sources = (z, z + 1 - 2 * (z % 2), 2 - low, 3 * (1 - low))
    flips = (0, 1, 2 + mid, 3 - mid)
    ways = (0, 1 - 2 * (z % 2), 1 - 2 * low, 1 - 2 * low)
    landings = (
        0,
        sources[1] + (PLANES - sources[1]) * (z % 2),
        sources[2] + (PLANES - sources[2]) * low * (1 - z % 2),
        sources[3],
    )
    is_mid, is_end = mid == 1, mid == 0
    crossed = (z, z + 1 - 2 * (z % 2), z + 2 - 4 * low, PLANES - 1 - z)
    aways = (0, 2 * (z % 2) - 1, 2 * low - 1, 2 * low - 1)
    has_left, has_right = z > 0, z < PLANES - 1
    wide = own.shape[1] // CHUNKS

    def cols(number):
        return pl.ds(pl.multiple_of(number * wide, wide), wide)

    def every(number):
        return pl.ds(0, CHUNKS * wide) if number is None else cols(number)

    def along(way):
        return {"sp": me + way * chips}

    def dispatch(source, number, way, slot, block=None):
        block = dense.at[source] if block is None else block
        return pltpu.make_async_remote_copy(
            src_ref=block.at[:, cols(number)],
            dst_ref=dense.at[source, :, cols(number)],
            send_sem=disp_sent.at[slot],
            recv_sem=disp_came.at[source, number],
            device_id=along(way),
            device_id_type=MESH,
        )

    def plane_copy(turn, number, place, places=1):
        return pltpu.make_async_remote_copy(
            src_ref=pick.at[turn, pl.ds(place * cap, places * cap), cols(number)],
            dst_ref=rows.at[turn, pl.ds(place * cap, places * cap), cols(number)],
            send_sem=plane_sent.at[0],
            recv_sem=plane_came.at[turn, number],
            device_id={"sp": flipped(me, place)},
            device_id_type=MESH,
        )

    def pair_copy(turn, number):
        return pltpu.make_async_remote_copy(
            src_ref=rows.at[turn, pl.ds(0, half), every(number)],
            dst_ref=rows.at[turn, pl.ds(half, half), every(number)],
            send_sem=pair_sent.at[0],
            recv_sem=pair_came.at[turn],
            device_id={"tp": other},
            device_id_type=MESH,
        )

    def share_copy(turn, number):
        return pltpu.make_async_remote_copy(
            src_ref=part.at[turn, pl.ds(half, half), cols(number)],
            dst_ref=given.at[turn, :, cols(number)],
            send_sem=part_sent.at[0],
            recv_sem=part_came.at[turn, number],
            device_id={"tp": other},
            device_id_type=MESH,
        )

    def back_copy(turn, number, place, places=1):
        return pltpu.make_async_remote_copy(
            src_ref=part.at[turn, pl.ds(place * cap, places * cap), cols(number)],
            dst_ref=ret.at[turn, pl.ds(place * cap, places * cap), cols(number)],
            send_sem=back_sent.at[0],
            recv_sem=back_came.at[turn, number],
            device_id={"sp": flipped(me, place)},
            device_id_type=MESH,
        )

    def chain_copy(turn, number, landing=None):
        landing = landings[turn] if landing is None else landing
        return pltpu.make_async_remote_copy(
            src_ref=zout.at[turn, :, cols(number)],
            dst_ref=zin.at[landing, :, cols(number)],
            send_sem=chain_sent.at[0],
            recv_sem=chain_came.at[landing, number],
            device_id=along(ways[turn]),
            device_id_type=MESH,
        )

    loads = [
        pltpu.make_async_copy(source.at[0], target, loaded.at[number])
        for number, (source, target) in enumerate(
            ((gate_in, gate_w), (up_in, up_w), (down_in, down_w))
        )
    ]
    for load in loads:
        load.start()

    barrier = pltpu.get_barrier_semaphore()
    for place in range(1, chips):
        pl.semaphore_signal(
            barrier, inc=1, device_id={"sp": flipped(me, place)}, device_id_type=MESH
        )
    pl.semaphore_signal(barrier, inc=1, device_id={"tp": other}, device_id_type=MESH)

    @pl.when(has_left)
    def _():
        pl.semaphore_signal(barrier, inc=1, device_id=along(-1), device_id_type=MESH)

    @pl.when(has_right)
    def _():
        pl.semaphore_signal(barrier, inc=1, device_id=along(1), device_id_type=MESH)

    pl.semaphore_wait(barrier, chips + (z + 2) // 3 + (PLANES + 1 - z) // 3)

    def send_own(number, carry):
        pl.when(has_left)(lambda: dispatch(z, number, -1, 0, own).start())
        pl.when(has_right)(lambda: dispatch(z, number, 1, 1, own).start())
        return carry

    lax.fori_loop(0, CHUNKS, send_own, 0)

    def select(turn, flip, block, number):
        chosen = jnp.dot(
            picks[flip], block[:, cols(number)], preferred_element_type=jnp.float32
        ).astype(jnp.bfloat16)
        rows[turn, pl.ds(0, cap), cols(number)] = chosen[:cap]
        pick[turn, :, cols(number)] = chosen
        for place in range(1, chips):
            plane_copy(turn, number, place).start()

    def arrive(turn, flip, number):
        source = crossed[flip]
        dispatch(source, number, 0, 0).wait_recv()
        pl.when(is_mid)(lambda: dispatch(source, number, aways[flip], 2).start())
        select(turn, flip, dense.at[source], number)

    def near(number):
        arrive(1, 1, number)
        pl.when(is_mid)(lambda: arrive(2, 3, number))

    def next_near(number):
        arrive(2 + mid, 2, number)

    def far(number):
        pl.when(is_end)(lambda: arrive(3, 3, number))

    def gather(turn):
        def step(number, carry):
            plane_copy(turn, number, 1, chips - 1).wait_recv()
            pair_copy(turn, number).start()
            return carry

        lax.fori_loop(0, CHUNKS, step, 0)
        if turn == 0:
            for load in loads:
                load.wait()

        pair_copy(turn, None).wait_recv()

    def first(turn, begin, end):
        narrow = min(256, gate_w.shape[1])

        def step(number, carry):
            columns = pl.ds(pl.multiple_of(number * narrow, narrow), narrow)
            gate = jnp.dot(rows[turn], gate_w[:, columns], preferred_element_type=jnp.float32)
            upper = jnp.dot(rows[turn], up_w[:, columns], preferred_element_type=jnp.float32)
            hidden[:, columns] = (jax.nn.silu(gate) * upper).astype(jnp.bfloat16)
            return carry

        blocks = gate_w.shape[1] // narrow
        lax.fori_loop(begin * blocks // CHUNKS, end * blocks // CHUNKS, step, 0)

    def second(turn, begin, end):
        def step(number, carry):
            part[turn, :, cols(number)] = jnp.dot(
                hidden[...], down_w[:, cols(number)], preferred_element_type=jnp.float32
            ).astype(jnp.bfloat16)
            share_copy(turn, number).start()
            return carry

        lax.fori_loop(begin, end, step, 0)

    def third(turn, begin, end):
        def step(number, carry):
            share_copy(turn, number).wait_recv()
            total = (
                part[turn, pl.ds(0, half), cols(number)].astype(jnp.float32)
                + given[turn, :, cols(number)].astype(jnp.float32)
            ).astype(jnp.bfloat16)
            part[turn, pl.ds(0, half), cols(number)] = total
            ret[turn, pl.ds(0, cap), cols(number)] = total[:cap]
            for place in range(1, chips):
                back_copy(turn, number, place).start()
            return carry

        lax.fori_loop(begin, end, step, 0)

    def combined(turn, number):
        back_copy(turn, number, 1, chips - 1).wait_recv()
        block = ret[turn, :, cols(number)]
        return jnp.dot(
            weights[flips[turn], 0], block, preferred_element_type=jnp.float32
        ) + jnp.dot(weights[flips[turn], 1], block, preferred_element_type=jnp.float32)

    def end_chain(turn, number):
        @pl.when(is_end)
        def _():
            zout[turn, :, cols(number)] = combined(turn, number).astype(jnp.bfloat16)
            chain_copy(turn, number).start()

    def mid_link(turn, number):
        partial = combined(turn, number)
        chain_copy(turn, number, sources[turn]).wait_recv()
        zout[turn, :, cols(number)] = (
            partial + zin[sources[turn], :, cols(number)].astype(jnp.float32)
        ).astype(jnp.bfloat16)
        chain_copy(turn, number).start()

    def run(*steps):
        for step, *rest in steps:
            step(*rest)

    G, F, U, T, C = gather, first, second, third, end_chain
    A, B, E = near, next_near, far
    for number in range(CHUNKS):
        select(0, 0, own, number)
    run((A, 0), (A, 1), (A, 2), (A, 3), (G, 0), (F, 0, 0, 8))
    run((A, 4), (A, 5), (U, 0, 0, 4), (A, 6), (U, 0, 4, 8), (A, 7), (B, 0))
    run((G, 1), (F, 1, 0, 4), (B, 1), (B, 2), (F, 1, 4, 8), (B, 3), (U, 1, 0, 4), (B, 4))
    run((U, 1, 4, 8), (B, 5), (T, 1, 0, 4), (B, 6), (T, 1, 4, 6), (B, 7), (T, 1, 6, 8), (C, 1, 0))
    run((E, 0), (C, 1, 1), (C, 1, 2), (E, 1), (C, 1, 3), (C, 1, 4), (G, 2), (F, 2, 0, 4), (E, 2))
    run((E, 3), (C, 1, 5), (C, 1, 6), (C, 1, 7), (F, 2, 4, 8), (E, 4), (U, 2, 0, 4), (E, 5))
    run((U, 2, 4, 8), (T, 2, 0, 2), (E, 6), (T, 2, 2, 4), (E, 7), (T, 2, 4, 8), (C, 2, 0), (C, 2, 1))
    run((C, 2, 2), (C, 2, 3), (G, 3), (F, 3, 0, 4), (C, 2, 4), (C, 2, 5), (C, 2, 6), (C, 2, 7))
    run((F, 3, 4, 8), (U, 3, 0, 4), (U, 3, 4, 8), (T, 3, 0, 8), (T, 0, 0, 8))
    for number in range(CHUNKS):
        end_chain(3, number)

    @pl.when(is_mid)
    def _():
        for number in range(CHUNKS):
            mid_link(2, number)
        for number in range(CHUNKS):
            mid_link(3, number)
            if number > 1:
                mid_link(1, number - 2)
        mid_link(1, CHUNKS - 2)
        mid_link(1, CHUNKS - 1)

    def finish(number, carry):
        out[:, cols(number)] = combined(0, number)

        def joined(landing):
            chain_copy(1, number, landing).wait_recv()
            out[:, cols(number)] += zin[landing, :, cols(number)].astype(jnp.float32)

        pl.when(has_left)(lambda: joined(z))
        pl.when(has_right)(lambda: joined(PLANES))
        return carry

    lax.fori_loop(0, CHUNKS, finish, 0)

    def sent(block, semaphore):
        return pltpu.make_async_remote_copy(
            src_ref=block,
            dst_ref=block,
            send_sem=semaphore.at[0],
            recv_sem=semaphore.at[0],
            device_id={"tp": other},
            device_id_type=MESH,
        )

    pl.when(has_left)(lambda: sent(own, disp_sent).wait_send())
    pl.when(has_right)(lambda: sent(own, disp_sent.at[pl.ds(1, 1)]).wait_send())
    pl.when(is_mid)(
        lambda: sent(dense.at[pl.ds(0, PLANES - 1)], disp_sent.at[pl.ds(2, 1)]).wait_send()
    )
    sent(rows.at[:, pl.ds(0, half)], pair_sent).wait_send()
    sent(given, part_sent).wait_send()
    sent(pick.at[:, pl.ds(0, half - cap)], plane_sent).wait_send()
    sent(ret.at[:, pl.ds(0, half - cap)], back_sent).wait_send()
    sent(zout.at[pl.ds(1, PLANES - 1)], chain_sent).wait_send()


def run_experts(own, picks, weights, expert_gate, expert_up, expert_down, count, cap):
    row_count, width = own.shape
    units = expert_gate.shape[2]
    chips = count // PLANES
    half = chips * cap
    dma = lambda *shape: pltpu.SemaphoreType.DMA(shape)
    vmem = pl.BlockSpec(memory_space=pltpu.VMEM)
    anywhere = pl.BlockSpec(memory_space=pl.ANY)
    held = jnp.bfloat16
    return pl.pallas_call(
        functools.partial(experts_kernel, count, cap),
        out_shape=jax.ShapeDtypeStruct((row_count, width), jnp.float32),
        in_specs=[vmem, vmem, vmem, anywhere, anywhere, anywhere],
        out_specs=vmem,
        scratch_shapes=[
            pltpu.VMEM((PLANES, row_count, width), held),
            pltpu.VMEM((PLANES, half, width), held),
            pltpu.VMEM((PLANES, 2 * half, width), held),
            pltpu.VMEM((PLANES, 2 * half, width), held),
            pltpu.VMEM((PLANES, half, width), held),
            pltpu.VMEM((2 * half, units), held),
            pltpu.VMEM((PLANES, half, width), held),
            pltpu.VMEM((PLANES, row_count, width), held),
            pltpu.VMEM((PLANES + 1, row_count, width), held),
            pltpu.VMEM((width, units), held),
            pltpu.VMEM((width, units), held),
            pltpu.VMEM((units, width), held),
            dma(3), dma(PLANES, CHUNKS),
            dma(1), dma(PLANES, CHUNKS),
            dma(1), dma(PLANES),
            dma(1), dma(PLANES, CHUNKS),
            dma(1), dma(PLANES, CHUNKS),
            dma(1), dma(PLANES + 1, CHUNKS),
            dma(3),
        ],
        compiler_params=pltpu.CompilerParams(
            collective_id=0, has_side_effects=True, vmem_limit_bytes=62 * 1024 * 1024
        ),
    )(own, picks, weights, expert_gate, expert_up, expert_down)


def from_behind(value, axis, steps):
    count = lax.axis_size(axis)
    first, last = (max(0, -steps), min(count, count - steps))
    return lax.ppermute(value, axis, [(source, source + steps) for source in range(first, last)])


def swap(value, axis, offset):
    count = lax.axis_size(axis)
    return lax.ppermute(value, axis, [(source, source ^ offset) for source in range(count)])


def on_device(
    residual_in,
    conv_values,
    conv_gates,
    conv_kernel,
    conv_bias,
    chan_gain,
    chan_shift,
    out_weight,
    norm_gain,
    route_ids,
    route_weights,
    expert_gate,
    expert_up,
    expert_down,
):
    taps_count = conv_kernel.shape[0]
    tok_count, local_chan = conv_values.shape
    tp_count = lax.axis_size("tp")
    all_chan = local_chan * tp_count
    core = lax.axis_index("tp")
    gated = (
        conv_values.astype(jnp.float32) * jax.nn.sigmoid(conv_gates.astype(jnp.float32))
    ).astype(jnp.bfloat16)
    earlier = from_behind(gated[tok_count - (taps_count - 1) :], "sp", 1)
    extended = jnp.concatenate([earlier, gated], 0).astype(jnp.float32)
    mixed = jnp.zeros((tok_count, local_chan), jnp.float32) + conv_bias[None, :]
    for tap_index in range(taps_count):
        mixed = (
            mixed + conv_kernel[tap_index][None, :] * extended[tap_index : tap_index + tok_count]
        )
    sums = jnp.stack([jnp.sum(mixed, 1), jnp.sum(mixed * mixed, 1)])
    sums = sums + swap(sums, "tp", 1)
    center = (sums[0] / all_chan)[:, None]
    spread = (sums[1] / all_chan)[:, None] - center * center
    normed = (mixed - center) * lax.rsqrt(spread + 1e-06) * chan_gain[None, :] + chan_shift[None, :]
    activated = jax.nn.silu(normed).astype(jnp.bfloat16)
    row_count = tok_count // tp_count
    low, high = activated[:row_count], activated[row_count:]
    kept = jnp.where(core == 0, low, high)
    given = swap(jnp.where(core == 0, high, low), "tp", 1)
    regrouped = jnp.concatenate(
        [jnp.where(core == 0, kept, given), jnp.where(core == 0, given, kept)], 1
    )
    projected = jnp.dot(regrouped, out_weight, preferred_element_type=jnp.float32)
    after_f = (residual_in.astype(jnp.float32) + projected).astype(jnp.bfloat16).astype(jnp.float32)
    normal_rows = (
        after_f
        * lax.rsqrt(jnp.mean(after_f * after_f, 1, keepdims=True) + 1e-06)
        * norm_gain[None, :]
    ).astype(jnp.bfloat16)
    sp_count = lax.axis_size("sp")
    experts_all = expert_gate.shape[0] * sp_count
    choose_count = route_ids.shape[1]
    slot_cap = max(2, (2 * choose_count * row_count + experts_all - 1) // experts_all)
    slot_cap = (slot_cap + 15) // 16 * 16
    onehot = (
        route_ids.reshape(-1)[:, None] == jnp.arange(experts_all, dtype=jnp.int32)[None, :]
    ).astype(jnp.int32)
    before = jnp.cumsum(onehot, 0) - onehot
    ranking = jnp.sum(before * onehot, 1).reshape(row_count, choose_count)
    chips = sp_count // PLANES
    half = chips * slot_cap
    me = lax.axis_index("sp")
    plane, place = me // chips, me % chips
    target_plane, target_place = route_ids // chips, route_ids % chips
    slot_ids = target_plane * half + (target_place ^ place) * slot_cap + ranking
    routing = jnp.concatenate([slot_ids.astype(jnp.float32), route_weights], 1).T
    routings = [routing] + [swap(routing, "sp", flip * chips) for flip in range(1, PLANES)]
    base = (plane * half).astype(jnp.float32)
    slots = lax.broadcasted_iota(jnp.int32, (half, 1), 0).astype(jnp.float32) + base
    lanes = lax.broadcasted_iota(jnp.int32, (1, half), 1).astype(jnp.float32) + base
    picks, weights = [], []
    for held in routings:
        ids, scales = held[:choose_count], held[choose_count:]
        chosen = functools.reduce(
            jnp.logical_or, [slots == ids[choice][None, :] for choice in range(choose_count)]
        )
        picks.append(chosen.astype(jnp.bfloat16))
        weighting = sum(
            jnp.where(lanes == ids[choice][:, None], scales[choice][:, None], 0.0)
            for choice in range(choose_count)
        )
        coarse_f = lax.reduce_precision(weighting, 8, 7)
        weights.append(
            jnp.stack([coarse_f.astype(jnp.bfloat16), (weighting - coarse_f).astype(jnp.bfloat16)])
        )
    summed = run_experts(
        normal_rows, jnp.stack(picks), jnp.stack(weights),
        expert_gate, expert_up, expert_down, sp_count, slot_cap,
    )
    combined = after_f + summed
    return combined.astype(jnp.bfloat16)


def solution(mesh):
    placed = (
        P(("sp", "tp"), None),
        P("sp", "tp"),
        P("sp", "tp"),
        P(None, "tp"),
        P("tp"),
        P("tp"),
        P("tp"),
        P(),
        P(),
        P(("sp", "tp"), None),
        P(("sp", "tp"), None),
        P("sp", None, "tp"),
        P("sp", None, "tp"),
        P("sp", "tp", None),
    )
    return jax.shard_map(
        on_device, mesh=mesh, in_specs=placed, out_specs=P(("sp", "tp"), None), check_vma=False
    )
```

```python
import functools

import jax
import jax.numpy as jnp
from jax import lax
from jax.experimental import pallas as pl
from jax.experimental.pallas import tpu as pltpu
from jax.sharding import PartitionSpec as P

PLANES = 4
CHUNKS = 8
MESH = pl.DeviceIdType.MESH


def flipped(index, offset):
    result, bit = index, 1
    while bit <= offset:
        if offset & bit:
            result = result + bit * (1 - 2 * ((index // bit) % 2))
        bit *= 2
    return result


def layer_kernel(
    count, cap, values, gates, taps, bias, gain, shift, norm_gain, ids, scales,
    residual_in, mix_in, gate_in, up_in, down_in, out,
    dense, pick, rows, part, given, hidden, ret, zout, zin, gate_w, up_w, down_w,
    extended, mixed, tail, stats, swapped, acted, route, picks, weights,
    disp_sent, disp_came, plane_sent, plane_came, pair_sent, pair_came, part_sent, part_came,
    back_sent, back_came, chain_sent, chain_came, loaded, mix_sent, mix_came,
):
    me, core = lax.axis_index("sp"), lax.axis_index("tp")
    other = 1 - core
    row_count, width = dense.shape[1], dense.shape[2]
    tok_count, chan = values.shape
    taps_count, groups = taps.shape[0], chan // 128
    pad = extended.shape[1] - tok_count
    after = zout.at[0]
    chips = count // PLANES
    half = chips * cap
    z = me // chips
    mid = ((z + 1) // 2) % 2
    low = z // 2
    sources = (z, z + 1 - 2 * (z % 2), 2 - low, 3 * (1 - low))
    flips = (0, 1, 2 + mid, 3 - mid)
    ways = (0, 1 - 2 * (z % 2), 1 - 2 * low, 1 - 2 * low)
    landings = (
        0,
        sources[1] + (PLANES - sources[1]) * (z % 2),
        sources[2] + (PLANES - sources[2]) * low * (1 - z % 2),
        sources[3],
    )
    is_mid, is_end = mid == 1, mid == 0
    crossed = (z, z + 1 - 2 * (z % 2), z + 2 - 4 * low, PLANES - 1 - z)
    aways = (0, 2 * (z % 2) - 1, 2 * low - 1, 2 * low - 1)
    has_left, has_right = z > 0, z < PLANES - 1
    wide = width // CHUNKS
    own = dense.at[z]

    def cols(number):
        return pl.ds(pl.multiple_of(number * wide, wide), wide)

    def every(number):
        return pl.ds(0, CHUNKS * wide) if number is None else cols(number)

    def along(way):
        return {"sp": me + way * chips}

    def dispatch(source, number, way, slot, block=None):
        block = dense.at[source] if block is None else block
        return pltpu.make_async_remote_copy(
            src_ref=block.at[:, cols(number)],
            dst_ref=dense.at[source, :, cols(number)],
            send_sem=disp_sent.at[slot],
            recv_sem=disp_came.at[source, number],
            device_id=along(way),
            device_id_type=MESH,
        )

    def plane_copy(turn, number, place, places=1):
        return pltpu.make_async_remote_copy(
            src_ref=pick.at[turn, pl.ds(place * cap, places * cap), cols(number)],
            dst_ref=rows.at[turn, pl.ds(place * cap, places * cap), cols(number)],
            send_sem=plane_sent.at[0],
            recv_sem=plane_came.at[turn, number],
            device_id={"sp": flipped(me, place)},
            device_id_type=MESH,
        )

    def pair_copy(turn, number):
        return pltpu.make_async_remote_copy(
            src_ref=rows.at[turn, pl.ds(0, half), every(number)],
            dst_ref=rows.at[turn, pl.ds(half, half), every(number)],
            send_sem=pair_sent.at[0],
            recv_sem=pair_came.at[turn],
            device_id={"tp": other},
            device_id_type=MESH,
        )

    def share_copy(turn, number):
        return pltpu.make_async_remote_copy(
            src_ref=part.at[turn, pl.ds(half, half), cols(number)],
            dst_ref=given.at[turn, :, cols(number)],
            send_sem=part_sent.at[0],
            recv_sem=part_came.at[turn, number],
            device_id={"tp": other},
            device_id_type=MESH,
        )

    def back_copy(turn, number, place, places=1):
        return pltpu.make_async_remote_copy(
            src_ref=part.at[turn, pl.ds(place * cap, places * cap), cols(number)],
            dst_ref=ret.at[turn, pl.ds(place * cap, places * cap), cols(number)],
            send_sem=back_sent.at[0],
            recv_sem=back_came.at[turn, number],
            device_id={"sp": flipped(me, place)},
            device_id_type=MESH,
        )

    def chain_copy(turn, number, landing=None):
        landing = landings[turn] if landing is None else landing
        return pltpu.make_async_remote_copy(
            src_ref=zout.at[turn, :, cols(number)],
            dst_ref=zin.at[landing, :, cols(number)],
            send_sem=chain_sent.at[0],
            recv_sem=chain_came.at[landing, number],
            device_id=along(ways[turn]),
            device_id_type=MESH,
        )

    loads = [
        pltpu.make_async_copy(source, target, loaded.at[number])
        for number, (source, target) in enumerate(
            (
                (gate_in.at[0], gate_w), (up_in.at[0], up_w), (down_in.at[0], down_w),
                (mix_in, down_w), (residual_in, after),
            )
        )
    ]
    early = loads[3:]
    loads = loads[:3]
    for load in early + loads[:2]:
        load.start()

    barrier = pltpu.get_barrier_semaphore()
    for place in range(1, chips):
        pl.semaphore_signal(
            barrier, inc=1, device_id={"sp": flipped(me, place)}, device_id_type=MESH
        )
    pl.semaphore_signal(barrier, inc=1, device_id={"tp": other}, device_id_type=MESH)

    for flip in range(1, PLANES):
        pl.semaphore_signal(
            barrier, inc=1, device_id={"sp": crossed[flip] * chips + me % chips}, device_id_type=MESH
        )

    def greet(step):
        pl.semaphore_signal(barrier, inc=1, device_id={"sp": me + step}, device_id_type=MESH)

    not_first, not_last = me > 0, me < count - 1
    pl.when(not_first)(lambda: greet(-1))
    pl.when(not_last)(lambda: greet(1))

    def gated(first_row, row_total, lanes):
        chosen = (pl.ds(first_row, row_total), lanes)
        return (
            values[chosen].astype(jnp.float32) * jax.nn.sigmoid(gates[chosen].astype(jnp.float32))
        ).astype(jnp.bfloat16)

    tail[0] = gated(tok_count - pad, pad, pl.ds(0, chan))
    pl.semaphore_wait(
        barrier,
        chips + PLANES - 1 + (me + count - 2) // (count - 1) + (2 * count - 3 - me) // (count - 1),
    )

    def mix_copy(source, target, number, device):
        return pltpu.make_async_remote_copy(
            src_ref=source,
            dst_ref=target,
            send_sem=mix_sent.at[number],
            recv_sem=mix_came.at[number],
            device_id=device,
            device_id_type=MESH,
        )

    halo = mix_copy(tail.at[0], tail.at[1], 0, {"sp": me + 1})
    moments = mix_copy(stats.at[0], stats.at[1], 1, {"tp": other})
    mine = pl.ds(pl.multiple_of(core * chan, chan), chan)
    exchange = mix_copy(swapped, acted.at[:, mine], 2, {"tp": other})
    routings = [
        mix_copy(
            route.at[0], route.at[flip], 2 + flip, {"sp": crossed[flip] * chips + me % chips}
        )
        for flip in range(1, PLANES)
    ]
    pl.when(not_last)(lambda: halo.start())

    experts_all = count
    expert_rows = lax.broadcasted_iota(jnp.int32, (experts_all, row_count), 0)
    named = [expert_rows == ids[choice : choice + 1, :] for choice in range(ids.shape[0])]
    onehot = sum(jnp.where(match, 1.0, 0.0) for match in named).astype(jnp.bfloat16)
    earlier = jnp.where(
        lax.broadcasted_iota(jnp.int32, (row_count, row_count), 0)
        < lax.broadcasted_iota(jnp.int32, (row_count, row_count), 1),
        1.0,
        0.0,
    ).astype(jnp.bfloat16)
    before = jnp.dot(onehot, earlier, preferred_element_type=jnp.float32)
    places = (
        (expert_rows // chips) * half
        + ((expert_rows % chips) ^ (me % chips)) * cap
    ).astype(jnp.float32) + before
    for choice, match in enumerate(named):
        route[0, choice : choice + 1, :] = jnp.sum(
            jnp.where(match, places, 0.0), 0, keepdims=True
        )
    lowest = ids.shape[0]
    route[0, lowest : 2 * lowest, :] = scales[...]
    for copy in routings:
        copy.start()

    for group in range(groups):
        extended[group, pl.ds(pad, tok_count), :] = gated(
            0, tok_count, pl.ds(group * 128, 128)
        ).astype(jnp.float32)

    @pl.when(not_first)
    def _():
        halo.wait_recv()
        for group in range(groups):
            extended[group, pl.ds(0, pad), :] = tail[1, :, pl.ds(group * 128, 128)].astype(
                jnp.float32
            )

    @pl.when(me == 0)
    def _():
        extended[:, pl.ds(0, pad), :] = jnp.zeros((groups, pad, 128), jnp.float32)

    block_rows = 64

    def convolve(number, carry):
        start = pl.multiple_of(number * block_rows, block_rows)
        total = jnp.zeros((block_rows, 128), jnp.float32)
        squares = total
        for group in range(groups):
            lanes = pl.ds(group * 128, 128)
            result = jnp.broadcast_to(bias[:, lanes], (block_rows, 128))
            for tap in range(taps_count):
                result = result + taps[tap : tap + 1, lanes] * (
                    extended[group, pl.ds(start + pad - taps_count + 1 + tap, block_rows), :]
                )
            mixed[group, pl.ds(start, block_rows), :] = result
            total = total + result
            squares = squares + result * result
        left = lax.broadcasted_iota(jnp.int32, (block_rows, 128), 1) < 64
        stats[0, pl.ds(start, block_rows), :] = jnp.where(
            left, jnp.sum(total, 1, keepdims=True), jnp.sum(squares, 1, keepdims=True)
        )
        return carry

    lax.fori_loop(0, tok_count // block_rows, convolve, 0)
    moments.start()
    def clear(landing):
        zin[landing] = jnp.zeros((row_count, width), jnp.bfloat16)

    pl.when(jnp.logical_not(has_left))(lambda: clear(z))
    pl.when(jnp.logical_not(has_right))(lambda: clear(PLANES))
    moments.wait_recv()

    def activate(half_index, store):
        start = pl.multiple_of(half_index * row_count, row_count)
        both = stats[0, pl.ds(start, row_count), :] + stats[1, pl.ds(start, row_count), :]
        center = both[:, 0:1] / (2 * chan)
        scale = lax.rsqrt(both[:, 64:65] / (2 * chan) - center * center + 1e-06)
        for group in range(groups):
            lanes = pl.ds(group * 128, 128)
            normed = (mixed[group, pl.ds(start, row_count), :] - center) * scale * gain[
                :, lanes
            ] + shift[:, lanes]
            store(group, jax.nn.silu(normed).astype(jnp.bfloat16))

    def store_swapped(group, value):
        swapped[:, pl.ds(group * 128, 128)] = value

    def store_mine(group, value):
        acted[:, pl.ds(pl.multiple_of(core * chan + group * 128, 128), 128)] = value

    activate(other, store_swapped)
    exchange.start()
    activate(core, store_mine)
    for load in early:
        load.wait()
    exchange.wait_recv()

    def project(number, carry):
        block = (
            after[:, cols(number)].astype(jnp.float32)
            + jnp.dot(acted[...], down_w[:, cols(number)], preferred_element_type=jnp.float32)
        ).astype(jnp.bfloat16)
        after[:, cols(number)] = block
        wider = block.astype(jnp.float32)
        return carry + jnp.sum(wider * wider, 1, keepdims=True)

    power = lax.fori_loop(0, CHUNKS, project, jnp.zeros((row_count, 1), jnp.float32))
    loads[2].start()
    level = lax.rsqrt(power / width + 1e-06)

    def send_own(number, carry):
        own[:, cols(number)] = (
            after[:, cols(number)].astype(jnp.float32) * level * norm_gain[:, cols(number)]
        ).astype(jnp.bfloat16)
        pl.when(has_left)(lambda: dispatch(z, number, -1, 0).start())
        pl.when(has_right)(lambda: dispatch(z, number, 1, 1).start())
        return carry

    lax.fori_loop(0, CHUNKS, send_own, 0)

    def place(flip):
        slots = (
            lax.broadcasted_iota(jnp.int32, (half, row_count), 0) + z * half
        ).astype(jnp.float32)
        matches = [slots == route[flip, choice : choice + 1, :] for choice in range(lowest)]
        picks[flip] = sum(jnp.where(match, 1.0, 0.0) for match in matches).astype(jnp.bfloat16)
        weighting = sum(
            jnp.where(match, route[flip, lowest + choice : lowest + choice + 1, :], 0.0)
            for choice, match in enumerate(matches)
        )
        coarse = weighting.astype(jnp.bfloat16)
        weights[flip, 0] = coarse
        weights[flip, 1] = (weighting - coarse.astype(jnp.float32)).astype(jnp.bfloat16)

    place(0)

    def select(turn, flip, block, number):
        chosen = jnp.dot(
            picks[flip], block[:, cols(number)], preferred_element_type=jnp.float32
        ).astype(jnp.bfloat16)
        rows[turn, pl.ds(0, cap), cols(number)] = chosen[:cap]
        pick[turn, :, cols(number)] = chosen
        for place in range(1, chips):
            plane_copy(turn, number, place).start()

    def arrive(turn, flip, number):
        source = crossed[flip]
        dispatch(source, number, 0, 0).wait_recv()
        pl.when(is_mid)(lambda: dispatch(source, number, aways[flip], 2).start())
        select(turn, flip, dense.at[source], number)

    def near(number):
        arrive(1, 1, number)
        pl.when(is_mid)(lambda: arrive(2, 3, number))

    def next_near(number):
        arrive(2 + mid, 2, number)

    def far(number):
        pl.when(is_end)(lambda: arrive(3, 3, number))

    def gather(turn):
        def step(number, carry):
            plane_copy(turn, number, 1, chips - 1).wait_recv()
            pair_copy(turn, number).start()
            return carry

        lax.fori_loop(0, CHUNKS, step, 0)
        if turn == 0:
            for load in loads:
                load.wait()

        pair_copy(turn, None).wait_recv()

    def first(turn, begin, end):
        narrow = min(256, gate_w.shape[1])

        def step(number, carry):
            columns = pl.ds(pl.multiple_of(number * narrow, narrow), narrow)
            gate = jnp.dot(rows[turn], gate_w[:, columns], preferred_element_type=jnp.float32)
            upper = jnp.dot(rows[turn], up_w[:, columns], preferred_element_type=jnp.float32)
            hidden[:, columns] = (jax.nn.silu(gate) * upper).astype(jnp.bfloat16)
            return carry

        blocks = gate_w.shape[1] // narrow
        lax.fori_loop(begin * blocks // CHUNKS, end * blocks // CHUNKS, step, 0)

    def second(turn, begin, end):
        def step(number, carry):
            part[turn, :, cols(number)] = jnp.dot(
                hidden[...], down_w[:, cols(number)], preferred_element_type=jnp.float32
            ).astype(jnp.bfloat16)
            share_copy(turn, number).start()
            return carry

        lax.fori_loop(begin, end, step, 0)

    def third(turn, begin, end):
        def step(number, carry):
            share_copy(turn, number).wait_recv()
            total = (
                part[turn, pl.ds(0, half), cols(number)].astype(jnp.float32)
                + given[turn, :, cols(number)].astype(jnp.float32)
            ).astype(jnp.bfloat16)
            part[turn, pl.ds(0, half), cols(number)] = total
            ret[turn, pl.ds(0, cap), cols(number)] = total[:cap]
            for place in range(1, chips):
                back_copy(turn, number, place).start()
            return carry

        lax.fori_loop(begin, end, step, 0)

    def combined(turn, number):
        back_copy(turn, number, 1, chips - 1).wait_recv()
        block = ret[turn, :, cols(number)]
        across = (((0,), (0,)), ((), ()))
        return lax.dot_general(
            weights[flips[turn], 0], block, across, preferred_element_type=jnp.float32
        ) + lax.dot_general(
            weights[flips[turn], 1], block, across, preferred_element_type=jnp.float32
        )

    def end_chain(turn, number):
        @pl.when(is_end)
        def _():
            zout[turn, :, cols(number)] = combined(turn, number).astype(jnp.bfloat16)
            chain_copy(turn, number).start()

    def mid_link(turn, number):
        partial = combined(turn, number)
        chain_copy(turn, number, sources[turn]).wait_recv()
        zout[turn, :, cols(number)] = (
            partial + zin[sources[turn], :, cols(number)].astype(jnp.float32)
        ).astype(jnp.bfloat16)
        chain_copy(turn, number).start()

    def run(*steps):
        for step, *rest in steps:
            step(*rest)

    G, F, U, T, C = gather, first, second, third, end_chain
    A, B, E = near, next_near, far
    for number in range(CHUNKS):
        select(0, 0, own, number)
    for flip in range(1, PLANES):
        routings[flip - 1].wait_recv()
        place(flip)
    run((A, 0), (A, 1), (A, 2), (A, 3), (G, 0), (F, 0, 0, 8))
    run((A, 4), (A, 5), (U, 0, 0, 4), (A, 6), (U, 0, 4, 8), (A, 7), (B, 0))
    run((G, 1), (F, 1, 0, 4), (B, 1), (B, 2), (F, 1, 4, 8), (B, 3), (U, 1, 0, 4), (B, 4))
    run((U, 1, 4, 8), (B, 5), (T, 1, 0, 4), (B, 6), (T, 1, 4, 6), (B, 7), (T, 1, 6, 8), (C, 1, 0))
    run((E, 0), (C, 1, 1), (C, 1, 2), (E, 1), (C, 1, 3), (C, 1, 4), (G, 2), (F, 2, 0, 4), (E, 2))
    run((E, 3), (C, 1, 5), (C, 1, 6), (C, 1, 7), (F, 2, 4, 8), (E, 4), (U, 2, 0, 4), (E, 5))
    run((U, 2, 4, 8), (T, 2, 0, 2), (E, 6), (T, 2, 2, 4), (E, 7), (T, 2, 4, 8), (C, 2, 0), (C, 2, 1))
    run((C, 2, 2), (C, 2, 3), (G, 3), (F, 3, 0, 4), (C, 2, 4), (C, 2, 5), (C, 2, 6), (C, 2, 7))
    run((F, 3, 4, 8), (U, 3, 0, 4), (U, 3, 4, 8), (T, 3, 0, 8), (T, 0, 0, 8))
    for number in range(CHUNKS):
        end_chain(3, number)

    @pl.when(is_mid)
    def _():
        for number in range(CHUNKS):
            mid_link(2, number)
        for number in range(CHUNKS):
            mid_link(3, number)
            if number > 1:
                mid_link(1, number - 2)
        mid_link(1, CHUNKS - 2)
        mid_link(1, CHUNKS - 1)

    def finish(number, carry):
        total = after[:, cols(number)].astype(jnp.float32) + combined(0, number)
        pl.when(has_left)(lambda: chain_copy(1, number, z).wait_recv())
        pl.when(has_right)(lambda: chain_copy(1, number, PLANES).wait_recv())
        out[:, cols(number)] = (
            total
            + zin[z, :, cols(number)].astype(jnp.float32)
            + zin[PLANES, :, cols(number)].astype(jnp.float32)
        ).astype(jnp.bfloat16)
        return carry

    lax.fori_loop(0, CHUNKS, finish, 0)

    def sent(block, semaphore):
        return pltpu.make_async_remote_copy(
            src_ref=block,
            dst_ref=block,
            send_sem=semaphore.at[0],
            recv_sem=semaphore.at[0],
            device_id={"tp": other},
            device_id_type=MESH,
        )

    pl.when(not_last)(lambda: halo.wait_send())
    moments.wait_send()
    exchange.wait_send()
    for copy in routings:
        copy.wait_send()
    pl.when(has_left)(lambda: sent(own, disp_sent).wait_send())
    pl.when(has_right)(lambda: sent(own, disp_sent.at[pl.ds(1, 1)]).wait_send())
    pl.when(is_mid)(
        lambda: sent(dense.at[pl.ds(0, PLANES - 1)], disp_sent.at[pl.ds(2, 1)]).wait_send()
    )
    sent(rows.at[:, pl.ds(0, half)], pair_sent).wait_send()
    sent(given, part_sent).wait_send()
    sent(pick.at[:, pl.ds(0, half - cap)], plane_sent).wait_send()
    sent(ret.at[:, pl.ds(0, half - cap)], back_sent).wait_send()
    sent(zout.at[pl.ds(1, PLANES - 1)], chain_sent).wait_send()


def run_layer(
    values, gates, taps, bias, gain, shift, norm_gain, ids, scales,
    residual_in, out_weight, expert_gate, expert_up, expert_down, count, cap,
):
    row_count, width = residual_in.shape
    tok_count, chan = values.shape
    units = expert_gate.shape[2]
    chips = count // PLANES
    half = chips * cap
    pad = (taps.shape[0] + 14) // 16 * 16
    groups = chan // 128
    choose_count = ids.shape[0]
    dma = lambda *shape: pltpu.SemaphoreType.DMA(shape)
    vmem = pl.BlockSpec(memory_space=pltpu.VMEM)
    anywhere = pl.BlockSpec(memory_space=pl.ANY)
    held = jnp.bfloat16
    return pl.pallas_call(
        functools.partial(layer_kernel, count, cap),
        out_shape=jax.ShapeDtypeStruct((row_count, width), held),
        in_specs=[vmem] * 9 + [anywhere] * 5,
        out_specs=vmem,
        scratch_shapes=[
            pltpu.VMEM((PLANES, row_count, width), held),
            pltpu.VMEM((PLANES, half, width), held),
            pltpu.VMEM((PLANES, 2 * half, width), held),
            pltpu.VMEM((PLANES, 2 * half, width), held),
            pltpu.VMEM((PLANES, half, width), held),
            pltpu.VMEM((2 * half, units), held),
            pltpu.VMEM((PLANES, half, width), held),
            pltpu.VMEM((PLANES, row_count, width), held),
            pltpu.VMEM((PLANES + 1, row_count, width), held),
            pltpu.VMEM((width, units), held),
            pltpu.VMEM((width, units), held),
            pltpu.VMEM((units, width), held),
            pltpu.VMEM((groups, pad + tok_count, 128), jnp.float32),
            pltpu.VMEM((groups, tok_count, 128), jnp.float32),
            pltpu.VMEM((2, pad, chan), held),
            pltpu.VMEM((2, tok_count, 128), jnp.float32),
            pltpu.VMEM((row_count, chan), held),
            pltpu.VMEM((row_count, 2 * chan), held),
            pltpu.VMEM((PLANES, 2 * choose_count, row_count), jnp.float32),
            pltpu.VMEM((PLANES, half, row_count), held),
            pltpu.VMEM((PLANES, 2, half, row_count), held),
            dma(3), dma(PLANES, CHUNKS),
            dma(1), dma(PLANES, CHUNKS),
            dma(1), dma(PLANES),
            dma(1), dma(PLANES, CHUNKS),
            dma(1), dma(PLANES, CHUNKS),
            dma(1), dma(PLANES + 1, CHUNKS),
            dma(5), dma(2 + PLANES), dma(2 + PLANES),
        ],
        compiler_params=pltpu.CompilerParams(
            collective_id=0, has_side_effects=True, vmem_limit_bytes=63 * 1024 * 1024
        ),
    )(
        values, gates, taps, bias, gain, shift, norm_gain, ids, scales,
        residual_in, out_weight, expert_gate, expert_up, expert_down,
    )


def on_device(
    residual_in,
    conv_values,
    conv_gates,
    conv_kernel,
    conv_bias,
    chan_gain,
    chan_shift,
    out_weight,
    norm_gain,
    route_ids,
    route_weights,
    expert_gate,
    expert_up,
    expert_down,
):
    sp_count = lax.axis_size("sp")
    experts_all = expert_gate.shape[0] * sp_count
    choose_count, row_count = route_ids.shape[1], residual_in.shape[0]
    slot_cap = max(2, (2 * choose_count * row_count + experts_all - 1) // experts_all)
    slot_cap = (slot_cap + 15) // 16 * 16
    return run_layer(
        conv_values,
        conv_gates,
        conv_kernel,
        conv_bias[None, :],
        chan_gain[None, :],
        chan_shift[None, :],
        norm_gain[None, :],
        route_ids.T,
        route_weights.T,
        residual_in,
        out_weight,
        expert_gate,
        expert_up,
        expert_down,
        sp_count,
        slot_cap,
    )


def solution(mesh):
    placed = (
        P(("sp", "tp"), None),
        P("sp", "tp"),
        P("sp", "tp"),
        P(None, "tp"),
        P("tp"),
        P("tp"),
        P("tp"),
        P(),
        P(),
        P(("sp", "tp"), None),
        P(("sp", "tp"), None),
        P("sp", None, "tp"),
        P("sp", None, "tp"),
        P("sp", "tp", None),
    )
    return jax.shard_map(
        on_device, mesh=mesh, in_specs=placed, out_specs=P(("sp", "tp"), None), check_vma=False
    )
```

```python
import functools

import jax
import jax.numpy as jnp
from jax import lax
from jax.experimental import pallas as pl
from jax.experimental.pallas import tpu as pltpu
from jax.sharding import PartitionSpec as P

PLANES = 4
CHUNKS = 8
MESH = pl.DeviceIdType.MESH


def flipped(index, offset):
    result, bit = index, 1
    while bit <= offset:
        if offset & bit:
            result = result + bit * (1 - 2 * ((index // bit) % 2))
        bit *= 2
    return result


def layer_kernel(
    count, cap, values, gates, taps, bias, gain, shift, norm_gain, ids, scales,
    residual_in, mix_in, gate_in, up_in, down_in, out,
    dense, pick, rows, part, given, hidden, ret, zout, zin, gate_w, up_w, down_w,
    extended, mixed, tail, stats, swapped, acted, route, picks, weights,
    disp_sent, disp_came, plane_sent, plane_came, pair_sent, pair_came, part_sent, part_came,
    back_sent, back_came, chain_sent, chain_came, loaded, mix_sent, mix_came,
):
    me, core = lax.axis_index("sp"), lax.axis_index("tp")
    other = 1 - core
    row_count, width = dense.shape[1], dense.shape[2]
    tok_count, chan = values.shape
    taps_count, groups = taps.shape[0], chan // 128
    pad = extended.shape[1] - tok_count
    after = zout.at[0]
    chips = count // PLANES
    half = chips * cap
    z = me // chips
    mid = ((z + 1) // 2) % 2
    low = z // 2
    sources = (z, z + 1 - 2 * (z % 2), 3 * (1 - low), 2 - low)
    flips = (0, 1, 3 - mid, 2 + mid)
    ways = (0, 1 - 2 * (z % 2), 1 - 2 * low, 1 - 2 * low)
    landings = (
        0,
        sources[1] + (PLANES - sources[1]) * (z % 2),
        sources[2],
        sources[3] + (PLANES - sources[3]) * low * (1 - z % 2),
    )
    inner = 1 - 2 * low
    is_mid, is_end = mid == 1, mid == 0
    crossed = (z, z + 1 - 2 * (z % 2), z + 2 - 4 * low, PLANES - 1 - z)
    aways = (0, 2 * (z % 2) - 1, 2 * low - 1, 2 * low - 1)
    has_left, has_right = z > 0, z < PLANES - 1
    wide = width // CHUNKS
    own = dense.at[z]

    def cols(number):
        return pl.ds(pl.multiple_of(number * wide, wide), wide)

    def pairs(number):
        return pl.ds(pl.multiple_of(number * 2 * wide, 2 * wide), 2 * wide)

    def every(number):
        return pl.ds(0, CHUNKS * wide) if number is None else cols(number)

    def along(way):
        return {"sp": me + way * chips}

    def dispatch(source, number, way, slot, block=None):
        block = dense.at[source] if block is None else block
        return pltpu.make_async_remote_copy(
            src_ref=block.at[:, cols(number)],
            dst_ref=dense.at[source, :, cols(number)],
            send_sem=disp_sent.at[slot],
            recv_sem=disp_came.at[source, number],
            device_id=along(way),
            device_id_type=MESH,
        )

    def plane_copy(turn, number, place, places=1):
        return pltpu.make_async_remote_copy(
            src_ref=pick.at[turn, pl.ds(place * cap, places * cap), cols(number)],
            dst_ref=rows.at[turn, pl.ds(place * cap, places * cap), cols(number)],
            send_sem=plane_sent.at[0],
            recv_sem=plane_came.at[turn, number],
            device_id={"sp": flipped(me, place)},
            device_id_type=MESH,
        )

    def pair_copy(turn, number):
        return pltpu.make_async_remote_copy(
            src_ref=rows.at[turn, pl.ds(0, half), every(number)],
            dst_ref=rows.at[turn, pl.ds(half, half), every(number)],
            send_sem=pair_sent.at[0],
            recv_sem=pair_came.at[turn],
            device_id={"tp": other},
            device_id_type=MESH,
        )

    def share_copy(turn, number):
        return pltpu.make_async_remote_copy(
            src_ref=part.at[turn, pl.ds(half, half), cols(number)],
            dst_ref=given.at[turn, :, cols(number)],
            send_sem=part_sent.at[0],
            recv_sem=part_came.at[turn, number],
            device_id={"tp": other},
            device_id_type=MESH,
        )

    def back_copy(turn, number, place, places=1):
        return pltpu.make_async_remote_copy(
            src_ref=part.at[turn, pl.ds(place * cap, places * cap), cols(number)],
            dst_ref=ret.at[turn, pl.ds(place * cap, places * cap), cols(number)],
            send_sem=back_sent.at[0],
            recv_sem=back_came.at[turn, number],
            device_id={"sp": flipped(me, place)},
            device_id_type=MESH,
        )

    def chain_copy(turn, number, landing=None):
        landing = landings[turn] if landing is None else landing
        return pltpu.make_async_remote_copy(
            src_ref=zout.at[turn, :, cols(number)],
            dst_ref=zin.at[landing, :, cols(number)],
            send_sem=chain_sent.at[0],
            recv_sem=chain_came.at[landing, number],
            device_id=along(ways[turn]),
            device_id_type=MESH,
        )

    loads = [
        pltpu.make_async_copy(source, target, loaded.at[number])
        for number, (source, target) in enumerate(
            (
                (gate_in.at[0], gate_w), (up_in.at[0], up_w), (down_in.at[0], down_w),
                (mix_in, down_w), (residual_in, after),
            )
        )
    ]
    early = loads[3:]
    loads = loads[:3]
    for load in early + loads[:2]:
        load.start()

    barrier = pltpu.get_barrier_semaphore()
    for place in range(1, chips):
        pl.semaphore_signal(
            barrier, inc=1, device_id={"sp": flipped(me, place)}, device_id_type=MESH
        )
    pl.semaphore_signal(barrier, inc=1, device_id={"tp": other}, device_id_type=MESH)

    for flip in range(1, PLANES):
        pl.semaphore_signal(
            barrier, inc=1, device_id={"sp": crossed[flip] * chips + me % chips}, device_id_type=MESH
        )

    def greet(step):
        pl.semaphore_signal(barrier, inc=1, device_id={"sp": me + step}, device_id_type=MESH)

    not_first, not_last = me > 0, me < count - 1
    pl.when(not_first)(lambda: greet(-1))
    pl.when(not_last)(lambda: greet(1))

    def gated(first_row, row_total, lanes):
        chosen = (pl.ds(first_row, row_total), lanes)
        return (
            values[chosen].astype(jnp.float32) * jax.nn.sigmoid(gates[chosen].astype(jnp.float32))
        ).astype(jnp.bfloat16)

    tail[0] = gated(tok_count - pad, pad, pl.ds(0, chan))
    pl.semaphore_wait(
        barrier,
        chips + PLANES - 1 + (me + count - 2) // (count - 1) + (2 * count - 3 - me) // (count - 1),
    )

    def mix_copy(source, target, number, device):
        return pltpu.make_async_remote_copy(
            src_ref=source,
            dst_ref=target,
            send_sem=mix_sent.at[number],
            recv_sem=mix_came.at[number],
            device_id=device,
            device_id_type=MESH,
        )

    halo = mix_copy(tail.at[0], tail.at[1], 0, {"sp": me + 1})
    moments = mix_copy(stats.at[0], stats.at[1], 1, {"tp": other})
    mine = pl.ds(pl.multiple_of(core * chan, chan), chan)
    exchange = mix_copy(swapped, acted.at[:, mine], 2, {"tp": other})
    routings = [
        mix_copy(
            route.at[0], route.at[flip], 2 + flip, {"sp": crossed[flip] * chips + me % chips}
        )
        for flip in range(1, PLANES)
    ]
    pl.when(not_last)(lambda: halo.start())

    experts_all = count
    expert_rows = lax.broadcasted_iota(jnp.int32, (experts_all, row_count), 0)
    named = [expert_rows == ids[choice : choice + 1, :] for choice in range(ids.shape[0])]
    onehot = sum(jnp.where(match, 1.0, 0.0) for match in named).astype(jnp.bfloat16)
    earlier = jnp.where(
        lax.broadcasted_iota(jnp.int32, (row_count, row_count), 0)
        < lax.broadcasted_iota(jnp.int32, (row_count, row_count), 1),
        1.0,
        0.0,
    ).astype(jnp.bfloat16)
    before = jnp.dot(onehot, earlier, preferred_element_type=jnp.float32)
    places = (
        (expert_rows // chips) * half
        + ((expert_rows % chips) ^ (me % chips)) * cap
    ).astype(jnp.float32) + before
    for choice, match in enumerate(named):
        route[0, choice : choice + 1, :] = jnp.sum(
            jnp.where(match, places, 0.0), 0, keepdims=True
        )
    lowest = ids.shape[0]
    route[0, lowest : 2 * lowest, :] = scales[...]
    for copy in routings:
        copy.start()

    for group in range(groups):
        extended[group, pl.ds(pad, tok_count), :] = gated(
            0, tok_count, pl.ds(group * 128, 128)
        ).astype(jnp.float32)

    block_rows = 64

    def convolve(number, carry):
        start = pl.multiple_of(number * block_rows, block_rows)
        total = jnp.zeros((block_rows, 128), jnp.float32)
        squares = total
        for group in range(groups):
            lanes = pl.ds(group * 128, 128)
            result = jnp.broadcast_to(bias[:, lanes], (block_rows, 128))
            for tap in range(taps_count):
                result = result + taps[tap : tap + 1, lanes] * (
                    extended[group, pl.ds(start + pad - taps_count + 1 + tap, block_rows), :]
                )
            mixed[group, pl.ds(start, block_rows), :] = result
            total = total + result
            squares = squares + result * result
        left = lax.broadcasted_iota(jnp.int32, (block_rows, 128), 1) < 64
        stats[0, pl.ds(start, block_rows), :] = jnp.where(
            left, jnp.sum(total, 1, keepdims=True), jnp.sum(squares, 1, keepdims=True)
        )
        return carry

    lax.fori_loop(1, tok_count // block_rows, convolve, 0)

    @pl.when(not_first)
    def _():
        halo.wait_recv()
        for group in range(groups):
            extended[group, pl.ds(0, pad), :] = tail[1, :, pl.ds(group * 128, 128)].astype(
                jnp.float32
            )

    @pl.when(me == 0)
    def _():
        extended[:, pl.ds(0, pad), :] = jnp.zeros((groups, pad, 128), jnp.float32)

    convolve(0, 0)
    moments.start()
    def clear(landing):
        zin[landing] = jnp.zeros((row_count, width), jnp.bfloat16)

    pl.when(jnp.logical_not(has_left))(lambda: clear(z))
    pl.when(jnp.logical_not(has_right))(lambda: clear(PLANES))
    moments.wait_recv()

    def activate(half_index, store):
        start = pl.multiple_of(half_index * row_count, row_count)
        both = stats[0, pl.ds(start, row_count), :] + stats[1, pl.ds(start, row_count), :]
        center = both[:, 0:1] / (2 * chan)
        scale = lax.rsqrt(both[:, 64:65] / (2 * chan) - center * center + 1e-06)
        for group in range(groups):
            lanes = pl.ds(group * 128, 128)
            normed = (mixed[group, pl.ds(start, row_count), :] - center) * scale * gain[
                :, lanes
            ] + shift[:, lanes]
            store(group, jax.nn.silu(normed).astype(jnp.bfloat16))

    def store_swapped(group, value):
        swapped[:, pl.ds(group * 128, 128)] = value

    def store_mine(group, value):
        acted[:, pl.ds(pl.multiple_of(core * chan + group * 128, 128), 128)] = value

    activate(other, store_swapped)
    exchange.start()
    activate(core, store_mine)
    for load in early:
        load.wait()
    exchange.wait_recv()

    def project(number, carry):
        block = (
            after[:, pairs(number)].astype(jnp.float32)
            + jnp.dot(acted[...], down_w[:, pairs(number)], preferred_element_type=jnp.float32)
        ).astype(jnp.bfloat16)
        after[:, pairs(number)] = block
        wider = block.astype(jnp.float32)
        return carry + jnp.sum(wider * wider, 1, keepdims=True)

    power = lax.fori_loop(0, CHUNKS // 2, project, jnp.zeros((row_count, 1), jnp.float32))
    loads[2].start()
    level = lax.rsqrt(power / width + 1e-06)

    def send_own(number, carry):
        own[:, cols(number)] = (
            after[:, cols(number)].astype(jnp.float32) * level * norm_gain[:, cols(number)]
        ).astype(jnp.bfloat16)
        pl.when(is_mid)(lambda: dispatch(z, number, -inner, 0).start())
        pl.when(is_end)(lambda: dispatch(z, number, inner, 1).start())
        return carry

    lax.fori_loop(0, CHUNKS, send_own, 0)

    def send_inner():
        def step(number, carry):
            dispatch(z, number, inner, 1).start()
            return carry

        pl.when(is_mid)(lambda: lax.fori_loop(0, CHUNKS, step, None))

    def place(flip):
        slots = (
            lax.broadcasted_iota(jnp.int32, (half, row_count), 0) + z * half
        ).astype(jnp.float32)
        matches = [slots == route[flip, choice : choice + 1, :] for choice in range(lowest)]
        picks[flip] = sum(jnp.where(match, 1.0, 0.0) for match in matches).astype(jnp.bfloat16)
        weighting = sum(
            jnp.where(match, route[flip, lowest + choice : lowest + choice + 1, :], 0.0)
            for choice, match in enumerate(matches)
        )
        coarse = weighting.astype(jnp.bfloat16)
        weights[flip, 0] = coarse
        weights[flip, 1] = (weighting - coarse.astype(jnp.float32)).astype(jnp.bfloat16)

    place(0)

    def select(turn, flip, block, number):
        chosen = jnp.dot(
            picks[flip], block[:, cols(number)], preferred_element_type=jnp.float32
        ).astype(jnp.bfloat16)
        rows[turn, pl.ds(0, cap), cols(number)] = chosen[:cap]
        pick[turn, :, cols(number)] = chosen
        for place in range(1, chips):
            plane_copy(turn, number, place).start()

    def arrive(turn, flip, number):
        source = crossed[flip]
        dispatch(source, number, 0, 0).wait_recv()
        pl.when(is_mid)(lambda: dispatch(source, number, aways[flip], 2).start())
        select(turn, flip, dense.at[source], number)

    def near(number):
        arrive(1, 1, number)

    def mid_next(number):
        pl.when(is_mid)(lambda: arrive(2, 2, number))

    def across(number):
        arrive(2 + mid, 3, number)

    def far(number):
        pl.when(is_end)(lambda: arrive(3, 2, number))

    def gather(turn):
        def step(number, carry):
            plane_copy(turn, number, 1, chips - 1).wait_recv()
            pair_copy(turn, number).start()
            return carry

        lax.fori_loop(0, CHUNKS, step, 0)
        if turn == 0:
            for load in loads:
                load.wait()

        pair_copy(turn, None).wait_recv()

    def first(turn, begin, end):
        narrow = min(256, gate_w.shape[1])

        def step(number, carry):
            columns = pl.ds(pl.multiple_of(number * narrow, narrow), narrow)
            gate = jnp.dot(rows[turn], gate_w[:, columns], preferred_element_type=jnp.float32)
            upper = jnp.dot(rows[turn], up_w[:, columns], preferred_element_type=jnp.float32)
            hidden[:, columns] = (jax.nn.silu(gate) * upper).astype(jnp.bfloat16)
            return carry

        blocks = gate_w.shape[1] // narrow
        lax.fori_loop(begin * blocks // CHUNKS, end * blocks // CHUNKS, step, 0)

    def second(turn, begin, end):
        def step(number, carry):
            part[turn, :, pairs(number)] = jnp.dot(
                hidden[...], down_w[:, pairs(number)], preferred_element_type=jnp.float32
            ).astype(jnp.bfloat16)
            share_copy(turn, 2 * number).start()
            share_copy(turn, 2 * number + 1).start()
            return carry

        lax.fori_loop(begin // 2, end // 2, step, 0)

    def third(turn, begin, end):
        def step(number, carry):
            share_copy(turn, number).wait_recv()
            total = (
                part[turn, pl.ds(0, half), cols(number)].astype(jnp.float32)
                + given[turn, :, cols(number)].astype(jnp.float32)
            ).astype(jnp.bfloat16)
            part[turn, pl.ds(0, half), cols(number)] = total
            ret[turn, pl.ds(0, cap), cols(number)] = total[:cap]
            for place in range(1, chips):
                back_copy(turn, number, place).start()
            return carry

        lax.fori_loop(begin, end, step, 0)

    def combined(turn, number):
        back_copy(turn, number, 1, chips - 1).wait_recv()
        block = ret[turn, :, cols(number)]
        across = (((0,), (0,)), ((), ()))
        return lax.dot_general(
            weights[flips[turn], 0], block, across, preferred_element_type=jnp.float32
        ) + lax.dot_general(
            weights[flips[turn], 1], block, across, preferred_element_type=jnp.float32
        )

    def end_chain(turn, number):
        @pl.when(is_end)
        def _():
            zout[turn, :, cols(number)] = combined(turn, number).astype(jnp.bfloat16)
            chain_copy(turn, number).start()

    def mid_link(turn, number):
        partial = combined(turn, number)
        chain_copy(turn, number, sources[turn]).wait_recv()
        zout[turn, :, cols(number)] = (
            partial + zin[sources[turn], :, cols(number)].astype(jnp.float32)
        ).astype(jnp.bfloat16)
        chain_copy(turn, number).start()

    def run(*steps):
        for step, *rest in steps:
            step(*rest)

    G, F, U, T, C = gather, first, second, third, end_chain
    A, M, B, E = near, mid_next, across, far
    for number in range(CHUNKS):
        select(0, 0, own, number)
    for flip in range(1, PLANES):
        routings[flip - 1].wait_recv()
        place(flip)
    run((A, 0), (A, 1), (A, 2), (M, 0), (A, 3), (M, 1), (G, 0), (F, 0, 0, 8))
    run((A, 4), (M, 2), (A, 5), (M, 3), (U, 0, 0, 4), (A, 6), (M, 4), (U, 0, 4, 8), (A, 7))
    run((send_inner,), (M, 5), (B, 0), (M, 6), (M, 7))
    run((G, 1), (F, 1, 0, 4), (B, 1), (B, 2), (F, 1, 4, 8), (B, 3), (U, 1, 0, 4), (U, 1, 4, 8))
    run((B, 4), (T, 1, 0, 3), (B, 5), (T, 1, 3, 4), (B, 6), (T, 1, 4, 5), (C, 1, 0), (B, 7))
    run((T, 1, 5, 6), (C, 1, 1), (C, 1, 2), (E, 0), (T, 1, 6, 8), (C, 1, 3), (E, 1), (G, 2))
    run((F, 2, 0, 4), (C, 1, 4), (C, 1, 5), (E, 2), (E, 3), (F, 2, 4, 8), (U, 2, 0, 4), (C, 1, 6))
    run((E, 4), (U, 2, 4, 8), (T, 2, 0, 2), (C, 1, 7), (E, 5), (E, 6), (T, 2, 2, 4), (E, 7))
    run((T, 2, 4, 6), (C, 2, 0), (T, 2, 6, 8), (C, 2, 1), (C, 2, 2), (C, 2, 3), (G, 3), (F, 3, 0, 4))
    run((C, 2, 4), (C, 2, 5), (F, 3, 4, 8), (U, 3, 0, 4), (C, 2, 6), (U, 3, 4, 8), (T, 3, 0, 4))
    run((C, 2, 7), (T, 3, 4, 8), (T, 0, 0, 8))
    for number in range(CHUNKS):
        end_chain(3, number)

    @pl.when(is_mid)
    def _():
        for number in range(CHUNKS):
            mid_link(2, number)
            if number > 1:
                mid_link(1, number - 2)
        mid_link(1, CHUNKS - 2)
        mid_link(1, CHUNKS - 1)
        for number in range(CHUNKS):
            mid_link(3, number)

    def finish(number, carry):
        total = after[:, cols(number)].astype(jnp.float32) + combined(0, number)
        pl.when(has_left)(lambda: chain_copy(1, number, z).wait_recv())
        pl.when(has_right)(lambda: chain_copy(1, number, PLANES).wait_recv())
        out[:, cols(number)] = (
            total
            + zin[z, :, cols(number)].astype(jnp.float32)
            + zin[PLANES, :, cols(number)].astype(jnp.float32)
        ).astype(jnp.bfloat16)
        return carry

    lax.fori_loop(0, CHUNKS, finish, 0)

    def sent(block, semaphore):
        return pltpu.make_async_remote_copy(
            src_ref=block,
            dst_ref=block,
            send_sem=semaphore.at[0],
            recv_sem=semaphore.at[0],
            device_id={"tp": other},
            device_id_type=MESH,
        )

    pl.when(not_last)(lambda: halo.wait_send())
    moments.wait_send()
    exchange.wait_send()
    for copy in routings:
        copy.wait_send()
    pl.when(is_mid)(lambda: sent(own, disp_sent).wait_send())
    sent(own, disp_sent.at[pl.ds(1, 1)]).wait_send()
    pl.when(is_mid)(
        lambda: sent(dense.at[pl.ds(0, PLANES - 1)], disp_sent.at[pl.ds(2, 1)]).wait_send()
    )
    sent(rows.at[:, pl.ds(0, half)], pair_sent).wait_send()
    sent(given, part_sent).wait_send()
    sent(pick.at[:, pl.ds(0, half - cap)], plane_sent).wait_send()
    sent(ret.at[:, pl.ds(0, half - cap)], back_sent).wait_send()
    sent(zout.at[pl.ds(1, PLANES - 1)], chain_sent).wait_send()


def run_layer(
    values, gates, taps, bias, gain, shift, norm_gain, ids, scales,
    residual_in, out_weight, expert_gate, expert_up, expert_down, count, cap,
):
    row_count, width = residual_in.shape
    tok_count, chan = values.shape
    units = expert_gate.shape[2]
    chips = count // PLANES
    half = chips * cap
    pad = (taps.shape[0] + 14) // 16 * 16
    groups = chan // 128
    choose_count = ids.shape[0]
    dma = lambda *shape: pltpu.SemaphoreType.DMA(shape)
    vmem = pl.BlockSpec(memory_space=pltpu.VMEM)
    anywhere = pl.BlockSpec(memory_space=pl.ANY)
    held = jnp.bfloat16
    return pl.pallas_call(
        functools.partial(layer_kernel, count, cap),
        out_shape=jax.ShapeDtypeStruct((row_count, width), held),
        in_specs=[vmem] * 9 + [anywhere] * 5,
        out_specs=vmem,
        scratch_shapes=[
            pltpu.VMEM((PLANES, row_count, width), held),
            pltpu.VMEM((PLANES, half, width), held),
            pltpu.VMEM((PLANES, 2 * half, width), held),
            pltpu.VMEM((PLANES, 2 * half, width), held),
            pltpu.VMEM((PLANES, half, width), held),
            pltpu.VMEM((2 * half, units), held),
            pltpu.VMEM((PLANES, half, width), held),
            pltpu.VMEM((PLANES, row_count, width), held),
            pltpu.VMEM((PLANES + 1, row_count, width), held),
            pltpu.VMEM((width, units), held),
            pltpu.VMEM((width, units), held),
            pltpu.VMEM((units, width), held),
            pltpu.VMEM((groups, pad + tok_count, 128), jnp.float32),
            pltpu.VMEM((groups, tok_count, 128), jnp.float32),
            pltpu.VMEM((2, pad, chan), held),
            pltpu.VMEM((2, tok_count, 128), jnp.float32),
            pltpu.VMEM((row_count, chan), held),
            pltpu.VMEM((row_count, 2 * chan), held),
            pltpu.VMEM((PLANES, 2 * choose_count, row_count), jnp.float32),
            pltpu.VMEM((PLANES, half, row_count), held),
            pltpu.VMEM((PLANES, 2, half, row_count), held),
            dma(3), dma(PLANES, CHUNKS),
            dma(1), dma(PLANES, CHUNKS),
            dma(1), dma(PLANES),
            dma(1), dma(PLANES, CHUNKS),
            dma(1), dma(PLANES, CHUNKS),
            dma(1), dma(PLANES + 1, CHUNKS),
            dma(5), dma(2 + PLANES), dma(2 + PLANES),
        ],
        compiler_params=pltpu.CompilerParams(
            collective_id=0, has_side_effects=True, vmem_limit_bytes=63 * 1024 * 1024
        ),
    )(
        values, gates, taps, bias, gain, shift, norm_gain, ids, scales,
        residual_in, out_weight, expert_gate, expert_up, expert_down,
    )


def on_device(
    residual_in,
    conv_values,
    conv_gates,
    conv_kernel,
    conv_bias,
    chan_gain,
    chan_shift,
    out_weight,
    norm_gain,
    route_ids,
    route_weights,
    expert_gate,
    expert_up,
    expert_down,
):
    sp_count = lax.axis_size("sp")
    experts_all = expert_gate.shape[0] * sp_count
    choose_count, row_count = route_ids.shape[1], residual_in.shape[0]
    slot_cap = max(2, (2 * choose_count * row_count + experts_all - 1) // experts_all)
    slot_cap = (slot_cap + 15) // 16 * 16
    return run_layer(
        conv_values,
        conv_gates,
        conv_kernel,
        conv_bias[None, :],
        chan_gain[None, :],
        chan_shift[None, :],
        norm_gain[None, :],
        route_ids.T,
        route_weights.T,
        residual_in,
        out_weight,
        expert_gate,
        expert_up,
        expert_down,
        sp_count,
        slot_cap,
    )


def solution(mesh):
    placed = (
        P(("sp", "tp"), None),
        P("sp", "tp"),
        P("sp", "tp"),
        P(None, "tp"),
        P("tp"),
        P("tp"),
        P("tp"),
        P(),
        P(),
        P(("sp", "tp"), None),
        P(("sp", "tp"), None),
        P("sp", None, "tp"),
        P("sp", None, "tp"),
        P("sp", "tp", None),
    )
    return jax.shard_map(
        on_device, mesh=mesh, in_specs=placed, out_specs=P(("sp", "tp"), None), check_vma=False
    )
```

```python
import functools

import jax
import jax.numpy as jnp
from jax import lax
from jax.experimental import pallas as pl
from jax.experimental.pallas import tpu as pltpu
from jax.sharding import PartitionSpec as P

PLANES = 4
CHUNKS = 8
MESH = pl.DeviceIdType.MESH


def flipped(index, offset):
    result, bit = index, 1
    while bit <= offset:
        if offset & bit:
            result = result + bit * (1 - 2 * ((index // bit) % 2))
        bit *= 2
    return result


def layer_kernel(
    count, cap, values, gates, taps, bias, gain, shift, norm_gain, ids, scales,
    residual_in, mix_in, gate_in, up_in, down_in, out,
    dense, pick, rows, part, given, hidden, ret, zout, zin, gate_w, up_w, down_w,
    extended, mixed, tail, stats, swapped, acted, route, picks, weights, projected,
    disp_sent, disp_came, plane_sent, plane_came, pair_sent, pair_came, part_sent, part_came,
    back_sent, back_came, chain_sent, chain_came, loaded, mix_sent, mix_came,
):
    me, core = lax.axis_index("sp"), lax.axis_index("tp")
    other = 1 - core
    row_count, width = dense.shape[1], dense.shape[2]
    tok_count, chan = values.shape
    taps_count, groups = taps.shape[0], chan // 128
    pad = extended.shape[1] - tok_count
    after = zout.at[0]
    chips = count // PLANES
    half = chips * cap
    z = me // chips
    mid = ((z + 1) // 2) % 2
    low = z // 2
    sources = (z, z + 1 - 2 * (z % 2), 3 * (1 - low), 2 - low)
    flips = (0, 1, 3 - mid, 2 + mid)
    ways = (0, 1 - 2 * (z % 2), 1 - 2 * low, 1 - 2 * low)
    landings = (
        0,
        sources[1] + (PLANES - sources[1]) * (z % 2),
        sources[2],
        sources[3] + (PLANES - sources[3]) * low * (1 - z % 2),
    )
    inner = 1 - 2 * low
    is_mid, is_end = mid == 1, mid == 0
    crossed = (z, z + 1 - 2 * (z % 2), z + 2 - 4 * low, PLANES - 1 - z)
    aways = (0, 2 * (z % 2) - 1, 2 * low - 1, 2 * low - 1)
    has_left, has_right = z > 0, z < PLANES - 1
    wide = width // CHUNKS
    own = dense.at[z]

    def cols(number):
        return pl.ds(pl.multiple_of(number * wide, wide), wide)

    def pairs(number):
        return pl.ds(pl.multiple_of(number * 2 * wide, 2 * wide), 2 * wide)

    def every(number):
        return pl.ds(0, CHUNKS * wide) if number is None else cols(number)

    def along(way):
        return {"sp": me + way * chips}

    def dispatch(source, number, way, slot, block=None):
        block = dense.at[source] if block is None else block
        return pltpu.make_async_remote_copy(
            src_ref=block.at[:, cols(number)],
            dst_ref=dense.at[source, :, cols(number)],
            send_sem=disp_sent.at[slot],
            recv_sem=disp_came.at[source, number],
            device_id=along(way),
            device_id_type=MESH,
        )

    def plane_copy(turn, number, place, places=1):
        return pltpu.make_async_remote_copy(
            src_ref=pick.at[turn, pl.ds(place * cap, places * cap), cols(number)],
            dst_ref=rows.at[turn, pl.ds(place * cap, places * cap), cols(number)],
            send_sem=plane_sent.at[0],
            recv_sem=plane_came.at[turn, number],
            device_id={"sp": flipped(me, place)},
            device_id_type=MESH,
        )

    def pair_copy(turn, number):
        return pltpu.make_async_remote_copy(
            src_ref=rows.at[turn, pl.ds(0, half), every(number)],
            dst_ref=rows.at[turn, pl.ds(half, half), every(number)],
            send_sem=pair_sent.at[0],
            recv_sem=pair_came.at[turn],
            device_id={"tp": other},
            device_id_type=MESH,
        )

    def share_copy(turn, number):
        return pltpu.make_async_remote_copy(
            src_ref=part.at[turn, pl.ds(half, half), cols(number)],
            dst_ref=given.at[turn, :, cols(number)],
            send_sem=part_sent.at[0],
            recv_sem=part_came.at[turn, number],
            device_id={"tp": other},
            device_id_type=MESH,
        )

    def back_copy(turn, number, place, places=1):
        return pltpu.make_async_remote_copy(
            src_ref=part.at[turn, pl.ds(place * cap, places * cap), cols(number)],
            dst_ref=ret.at[turn, pl.ds(place * cap, places * cap), cols(number)],
            send_sem=back_sent.at[0],
            recv_sem=back_came.at[turn, number],
            device_id={"sp": flipped(me, place)},
            device_id_type=MESH,
        )

    def chain_copy(turn, number, landing=None):
        landing = landings[turn] if landing is None else landing
        return pltpu.make_async_remote_copy(
            src_ref=zout.at[turn, :, cols(number)],
            dst_ref=zin.at[landing, :, cols(number)],
            send_sem=chain_sent.at[0],
            recv_sem=chain_came.at[landing, number],
            device_id=along(ways[turn]),
            device_id_type=MESH,
        )

    loads = [
        pltpu.make_async_copy(source, target, loaded.at[number])
        for number, (source, target) in enumerate(
            (
                (gate_in.at[0], gate_w), (up_in.at[0], up_w), (down_in.at[0], down_w),
                (mix_in, down_w), (residual_in, after),
            )
        )
    ]
    early = loads[3:]
    loads = loads[:3]
    for load in early + loads[:2]:
        load.start()

    barrier = pltpu.get_barrier_semaphore()
    for place in range(1, chips):
        pl.semaphore_signal(
            barrier, inc=1, device_id={"sp": flipped(me, place)}, device_id_type=MESH
        )
    pl.semaphore_signal(barrier, inc=1, device_id={"tp": other}, device_id_type=MESH)

    for flip in range(1, PLANES):
        pl.semaphore_signal(
            barrier, inc=1, device_id={"sp": crossed[flip] * chips + me % chips}, device_id_type=MESH
        )

    def greet(step):
        pl.semaphore_signal(barrier, inc=1, device_id={"sp": me + step}, device_id_type=MESH)

    not_first, not_last = me > 0, me < count - 1
    pl.when(not_first)(lambda: greet(-1))
    pl.when(not_last)(lambda: greet(1))

    def gated(first_row, row_total, lanes):
        chosen = (pl.ds(first_row, row_total), lanes)
        return (
            values[chosen].astype(jnp.float32) * jax.nn.sigmoid(gates[chosen].astype(jnp.float32))
        ).astype(jnp.bfloat16)

    tail[0] = gated(tok_count - pad, pad, pl.ds(0, chan))
    pl.semaphore_wait(
        barrier,
        chips + PLANES - 1 + (me + count - 2) // (count - 1) + (2 * count - 3 - me) // (count - 1),
    )

    def mix_copy(source, target, number, device):
        return pltpu.make_async_remote_copy(
            src_ref=source,
            dst_ref=target,
            send_sem=mix_sent.at[number],
            recv_sem=mix_came.at[number],
            device_id=device,
            device_id_type=MESH,
        )

    halo = mix_copy(tail.at[0], tail.at[1], 0, {"sp": me + 1})
    moments = mix_copy(stats.at[0], stats.at[1], 1, {"tp": other})
    mine = pl.ds(pl.multiple_of(core * chan, chan), chan)
    exchange = mix_copy(swapped, acted.at[:, mine], 2, {"tp": other})
    routings = [
        mix_copy(
            route.at[0], route.at[flip], 2 + flip, {"sp": crossed[flip] * chips + me % chips}
        )
        for flip in range(1, PLANES)
    ]
    pl.when(not_last)(lambda: halo.start())

    experts_all = count
    expert_rows = lax.broadcasted_iota(jnp.int32, (experts_all, row_count), 0)
    named = [expert_rows == ids[choice : choice + 1, :] for choice in range(ids.shape[0])]
    onehot = sum(jnp.where(match, 1.0, 0.0) for match in named).astype(jnp.bfloat16)
    earlier = jnp.where(
        lax.broadcasted_iota(jnp.int32, (row_count, row_count), 0)
        < lax.broadcasted_iota(jnp.int32, (row_count, row_count), 1),
        1.0,
        0.0,
    ).astype(jnp.bfloat16)
    before = jnp.dot(onehot, earlier, preferred_element_type=jnp.float32)
    places = (
        (expert_rows // chips) * half
        + ((expert_rows % chips) ^ (me % chips)) * cap
    ).astype(jnp.float32) + before
    for choice, match in enumerate(named):
        route[0, choice : choice + 1, :] = jnp.sum(
            jnp.where(match, places, 0.0), 0, keepdims=True
        )
    lowest = ids.shape[0]
    route[0, lowest : 2 * lowest, :] = scales[...]
    for copy in routings:
        copy.start()

    for group in range(groups):
        extended[group, pl.ds(pad, tok_count), :] = gated(
            0, tok_count, pl.ds(group * 128, 128)
        ).astype(jnp.float32)

    block_rows = 64

    def convolve(number, carry):
        start = pl.multiple_of(number * block_rows, block_rows)
        total = jnp.zeros((block_rows, 128), jnp.float32)
        squares = total
        for group in range(groups):
            lanes = pl.ds(group * 128, 128)
            result = jnp.broadcast_to(bias[:, lanes], (block_rows, 128))
            for tap in range(taps_count):
                result = result + taps[tap : tap + 1, lanes] * (
                    extended[group, pl.ds(start + pad - taps_count + 1 + tap, block_rows), :]
                )
            mixed[group, pl.ds(start, block_rows), :] = result
            total = total + result
            squares = squares + result * result
        left = lax.broadcasted_iota(jnp.int32, (block_rows, 128), 1) < 64
        stats[0, pl.ds(start, block_rows), :] = jnp.where(
            left, jnp.sum(total, 1, keepdims=True), jnp.sum(squares, 1, keepdims=True)
        )
        return carry

    lax.fori_loop(1, tok_count // block_rows, convolve, 0)

    @pl.when(not_first)
    def _():
        halo.wait_recv()
        for group in range(groups):
            extended[group, pl.ds(0, pad), :] = tail[1, :, pl.ds(group * 128, 128)].astype(
                jnp.float32
            )

    @pl.when(me == 0)
    def _():
        extended[:, pl.ds(0, pad), :] = jnp.zeros((groups, pad, 128), jnp.float32)

    convolve(0, 0)
    moments.start()
    def clear(landing):
        zin[landing] = jnp.zeros((row_count, width), jnp.bfloat16)

    pl.when(jnp.logical_not(has_left))(lambda: clear(z))
    pl.when(jnp.logical_not(has_right))(lambda: clear(PLANES))
    moments.wait_recv()

    def activate(half_index, store):
        start = pl.multiple_of(half_index * row_count, row_count)
        both = stats[0, pl.ds(start, row_count), :] + stats[1, pl.ds(start, row_count), :]
        center = both[:, 0:1] / (2 * chan)
        scale = lax.rsqrt(both[:, 64:65] / (2 * chan) - center * center + 1e-06)
        for group in range(groups):
            lanes = pl.ds(group * 128, 128)
            normed = (mixed[group, pl.ds(start, row_count), :] - center) * scale * gain[
                :, lanes
            ] + shift[:, lanes]
            store(group, jax.nn.silu(normed).astype(jnp.bfloat16))

    def store_swapped(group, value):
        swapped[:, pl.ds(group * 128, 128)] = value

    def store_mine(group, value):
        acted[:, pl.ds(pl.multiple_of(core * chan + group * 128, 128), 128)] = value

    activate(other, store_swapped)
    exchange.start()
    activate(core, store_mine)
    for load in early:
        load.wait()
    ours = pl.ds(pl.multiple_of(core * chan, chan), chan)
    theirs = pl.ds(pl.multiple_of(other * chan, chan), chan)

    def half_project(number, carry):
        projected[:, pairs(number)] = after[:, pairs(number)].astype(jnp.float32) + jnp.dot(
            acted[:, ours], down_w[ours, pairs(number)], preferred_element_type=jnp.float32
        )
        return carry

    lax.fori_loop(0, CHUNKS // 2, half_project, 0)
    exchange.wait_recv()

    def project(number, carry):
        block = (
            projected[:, pairs(number)]
            + jnp.dot(
                acted[:, theirs], down_w[theirs, pairs(number)], preferred_element_type=jnp.float32
            )
        ).astype(jnp.bfloat16)
        after[:, pairs(number)] = block
        wider = block.astype(jnp.float32)
        return carry + jnp.sum(wider * wider, 1, keepdims=True)

    power = lax.fori_loop(0, CHUNKS // 2, project, jnp.zeros((row_count, 1), jnp.float32))
    loads[2].start()
    level = lax.rsqrt(power / width + 1e-06)

    def send_own(number, carry):
        own[:, cols(number)] = (
            after[:, cols(number)].astype(jnp.float32) * level * norm_gain[:, cols(number)]
        ).astype(jnp.bfloat16)
        pl.when(is_mid)(lambda: dispatch(z, number, -inner, 0).start())
        pl.when(is_end)(lambda: dispatch(z, number, inner, 1).start())
        return carry

    lax.fori_loop(0, CHUNKS, send_own, 0)

    def send_inner():
        def step(number, carry):
            dispatch(z, number, inner, 1).start()
            return carry

        pl.when(is_mid)(lambda: lax.fori_loop(0, CHUNKS, step, None))

    def place(flip):
        slots = (
            lax.broadcasted_iota(jnp.int32, (half, row_count), 0) + z * half
        ).astype(jnp.float32)
        matches = [slots == route[flip, choice : choice + 1, :] for choice in range(lowest)]
        picks[flip] = sum(jnp.where(match, 1.0, 0.0) for match in matches).astype(jnp.bfloat16)
        weighting = sum(
            jnp.where(match, route[flip, lowest + choice : lowest + choice + 1, :], 0.0)
            for choice, match in enumerate(matches)
        )
        coarse = weighting.astype(jnp.bfloat16)
        weights[flip, 0] = coarse
        weights[flip, 1] = (weighting - coarse.astype(jnp.float32)).astype(jnp.bfloat16)

    place(0)

    def select(turn, flip, block, number):
        chosen = jnp.dot(
            picks[flip], block[:, cols(number)], preferred_element_type=jnp.float32
        ).astype(jnp.bfloat16)
        rows[turn, pl.ds(0, cap), cols(number)] = chosen[:cap]
        pick[turn, :, cols(number)] = chosen
        for place in range(1, chips):
            plane_copy(turn, number, place).start()

    def arrive(turn, flip, number):
        source = crossed[flip]
        dispatch(source, number, 0, 0).wait_recv()
        pl.when(is_mid)(lambda: dispatch(source, number, aways[flip], 2).start())
        select(turn, flip, dense.at[source], number)

    def near(number):
        arrive(1, 1, number)

    def mid_next(number):
        pl.when(is_mid)(lambda: arrive(2, 2, number))

    def across(number):
        arrive(2 + mid, 3, number)

    def far(number):
        pl.when(is_end)(lambda: arrive(3, 2, number))

    def gather(turn):
        def step(number, carry):
            plane_copy(turn, number, 1, chips - 1).wait_recv()
            pair_copy(turn, number).start()
            return carry

        lax.fori_loop(0, CHUNKS, step, 0)
        if turn == 0:
            for load in loads:
                load.wait()

        pair_copy(turn, None).wait_recv()

    def first(turn, begin, end):
        narrow = min(256, gate_w.shape[1])

        def step(number, carry):
            columns = pl.ds(pl.multiple_of(number * narrow, narrow), narrow)
            gate = jnp.dot(rows[turn], gate_w[:, columns], preferred_element_type=jnp.float32)
            upper = jnp.dot(rows[turn], up_w[:, columns], preferred_element_type=jnp.float32)
            hidden[:, columns] = (jax.nn.silu(gate) * upper).astype(jnp.bfloat16)
            return carry

        blocks = gate_w.shape[1] // narrow
        lax.fori_loop(begin * blocks // CHUNKS, end * blocks // CHUNKS, step, 0)

    def second(turn, begin, end):
        def step(number, carry):
            part[turn, :, pairs(number)] = jnp.dot(
                hidden[...], down_w[:, pairs(number)], preferred_element_type=jnp.float32
            ).astype(jnp.bfloat16)
            share_copy(turn, 2 * number).start()
            share_copy(turn, 2 * number + 1).start()
            return carry

        lax.fori_loop(begin // 2, end // 2, step, 0)

    def third(turn, begin, end):
        def step(number, carry):
            share_copy(turn, number).wait_recv()
            total = (
                part[turn, pl.ds(0, half), cols(number)].astype(jnp.float32)
                + given[turn, :, cols(number)].astype(jnp.float32)
            ).astype(jnp.bfloat16)
            part[turn, pl.ds(0, half), cols(number)] = total
            ret[turn, pl.ds(0, cap), cols(number)] = total[:cap]
            for place in range(1, chips):
                back_copy(turn, number, place).start()
            return carry

        lax.fori_loop(begin, end, step, 0)

    def combined(turn, number):
        back_copy(turn, number, 1, chips - 1).wait_recv()
        block = ret[turn, :, cols(number)]
        across = (((0,), (0,)), ((), ()))
        return lax.dot_general(
            weights[flips[turn], 0], block, across, preferred_element_type=jnp.float32
        ) + lax.dot_general(
            weights[flips[turn], 1], block, across, preferred_element_type=jnp.float32
        )

    def end_chain(turn, number):
        @pl.when(is_end)
        def _():
            zout[turn, :, cols(number)] = combined(turn, number).astype(jnp.bfloat16)
            chain_copy(turn, number).start()

    def mid_link(turn, number):
        partial = combined(turn, number)
        chain_copy(turn, number, sources[turn]).wait_recv()
        zout[turn, :, cols(number)] = (
            partial + zin[sources[turn], :, cols(number)].astype(jnp.float32)
        ).astype(jnp.bfloat16)
        chain_copy(turn, number).start()

    def run(*steps):
        for step, *rest in steps:
            step(*rest)

    G, F, U, T, C = gather, first, second, third, end_chain
    A, M, B, E = near, mid_next, across, far

    def R(turn, number):
        pl.when(is_mid)(lambda: mid_link(turn, number))

    for number in range(CHUNKS):
        select(0, 0, own, number)
    for flip in range(1, PLANES):
        routings[flip - 1].wait_recv()
        place(flip)
    run((A, 0), (A, 1), (A, 2), (M, 0), (A, 3), (M, 1), (G, 0), (F, 0, 0, 8))
    run((A, 4), (M, 2), (A, 5), (M, 3), (U, 0, 0, 4), (A, 6), (M, 4), (U, 0, 4, 8), (A, 7))
    run((send_inner,), (M, 5), (M, 6), (M, 7), (G, 1), (F, 1, 0, 4), (B, 0), (B, 1), (B, 2))
    run((F, 1, 4, 8), (B, 3), (U, 1, 0, 4), (B, 4), (T, 1, 0, 2), (U, 1, 4, 8), (T, 1, 2, 3), (B, 5))
    run((T, 1, 3, 4), (B, 6), (T, 1, 4, 5), (C, 1, 0), (B, 7))
    run((T, 1, 5, 6), (C, 1, 1), (C, 1, 2), (E, 0), (T, 1, 6, 8), (C, 1, 3), (E, 1), (G, 2))
    run((F, 2, 0, 4), (C, 1, 4), (C, 1, 5), (E, 2), (E, 3), (F, 2, 4, 8), (U, 2, 0, 4), (C, 1, 6))
    run((E, 4), (T, 2, 0, 2), (U, 2, 4, 8), (T, 2, 2, 4), (C, 1, 7), (E, 5), (E, 6), (E, 7))
    run((T, 2, 4, 6), (C, 2, 0), (T, 2, 6, 8), (C, 2, 1), (C, 2, 2), (C, 2, 3), (G, 3), (F, 3, 0, 4))
    run((C, 2, 4), (C, 2, 5), (F, 3, 4, 8), (R, 2, 0), (U, 3, 0, 4))
    run((C, 2, 6), (T, 3, 0, 2), (R, 2, 1), (U, 3, 4, 8), (T, 3, 2, 4), (C, 2, 7), (T, 3, 4, 8))
    run((R, 2, 2), (T, 0, 0, 8))
    for number in range(CHUNKS):
        end_chain(3, number)

    @pl.when(is_mid)
    def _():
        for number in range(CHUNKS):
            if number > 2:
                mid_link(2, number)
                mid_link(1, number - 3)
        for number in range(CHUNKS):
            mid_link(3, number)
            if number < 3:
                mid_link(1, CHUNKS - 3 + number)

    def finish(number, carry):
        total = after[:, cols(number)].astype(jnp.float32) + combined(0, number)
        pl.when(has_left)(lambda: chain_copy(1, number, z).wait_recv())
        pl.when(has_right)(lambda: chain_copy(1, number, PLANES).wait_recv())
        out[:, cols(number)] = (
            total
            + zin[z, :, cols(number)].astype(jnp.float32)
            + zin[PLANES, :, cols(number)].astype(jnp.float32)
        ).astype(jnp.bfloat16)
        return carry

    lax.fori_loop(0, CHUNKS, finish, 0)

    def sent(block, semaphore):
        return pltpu.make_async_remote_copy(
            src_ref=block,
            dst_ref=block,
            send_sem=semaphore.at[0],
            recv_sem=semaphore.at[0],
            device_id={"tp": other},
            device_id_type=MESH,
        )

    pl.when(not_last)(lambda: halo.wait_send())
    moments.wait_send()
    exchange.wait_send()
    for copy in routings:
        copy.wait_send()
    pl.when(is_mid)(lambda: sent(own, disp_sent).wait_send())
    sent(own, disp_sent.at[pl.ds(1, 1)]).wait_send()
    pl.when(is_mid)(
        lambda: sent(dense.at[pl.ds(0, PLANES - 1)], disp_sent.at[pl.ds(2, 1)]).wait_send()
    )
    sent(rows.at[:, pl.ds(0, half)], pair_sent).wait_send()
    sent(given, part_sent).wait_send()
    sent(pick.at[:, pl.ds(0, half - cap)], plane_sent).wait_send()
    sent(ret.at[:, pl.ds(0, half - cap)], back_sent).wait_send()
    sent(zout.at[pl.ds(1, PLANES - 1)], chain_sent).wait_send()


def run_layer(
    values, gates, taps, bias, gain, shift, norm_gain, ids, scales,
    residual_in, out_weight, expert_gate, expert_up, expert_down, count, cap,
):
    row_count, width = residual_in.shape
    tok_count, chan = values.shape
    units = expert_gate.shape[2]
    chips = count // PLANES
    half = chips * cap
    pad = (taps.shape[0] + 14) // 16 * 16
    groups = chan // 128
    choose_count = ids.shape[0]
    dma = lambda *shape: pltpu.SemaphoreType.DMA(shape)
    vmem = pl.BlockSpec(memory_space=pltpu.VMEM)
    anywhere = pl.BlockSpec(memory_space=pl.ANY)
    held = jnp.bfloat16
    return pl.pallas_call(
        functools.partial(layer_kernel, count, cap),
        out_shape=jax.ShapeDtypeStruct((row_count, width), held),
        in_specs=[vmem] * 9 + [anywhere] * 5,
        out_specs=vmem,
        scratch_shapes=[
            pltpu.VMEM((PLANES, row_count, width), held),
            pltpu.VMEM((PLANES, half, width), held),
            pltpu.VMEM((PLANES, 2 * half, width), held),
            pltpu.VMEM((PLANES, 2 * half, width), held),
            pltpu.VMEM((PLANES, half, width), held),
            pltpu.VMEM((2 * half, units), held),
            pltpu.VMEM((PLANES, half, width), held),
            pltpu.VMEM((PLANES, row_count, width), held),
            pltpu.VMEM((PLANES + 1, row_count, width), held),
            pltpu.VMEM((width, units), held),
            pltpu.VMEM((width, units), held),
            pltpu.VMEM((units, width), held),
            pltpu.VMEM((groups, pad + tok_count, 128), jnp.float32),
            pltpu.VMEM((groups, tok_count, 128), jnp.float32),
            pltpu.VMEM((2, pad, chan), held),
            pltpu.VMEM((2, tok_count, 128), jnp.float32),
            pltpu.VMEM((row_count, chan), held),
            pltpu.VMEM((row_count, 2 * chan), held),
            pltpu.VMEM((PLANES, 2 * choose_count, row_count), jnp.float32),
            pltpu.VMEM((PLANES, half, row_count), held),
            pltpu.VMEM((PLANES, 2, half, row_count), held),
            pltpu.VMEM((row_count, width), jnp.float32),
            dma(3), dma(PLANES, CHUNKS),
            dma(1), dma(PLANES, CHUNKS),
            dma(1), dma(PLANES),
            dma(1), dma(PLANES, CHUNKS),
            dma(1), dma(PLANES, CHUNKS),
            dma(1), dma(PLANES + 1, CHUNKS),
            dma(5), dma(2 + PLANES), dma(2 + PLANES),
        ],
        compiler_params=pltpu.CompilerParams(
            collective_id=0, has_side_effects=True, vmem_limit_bytes=63 * 1024 * 1024
        ),
    )(
        values, gates, taps, bias, gain, shift, norm_gain, ids, scales,
        residual_in, out_weight, expert_gate, expert_up, expert_down,
    )


def on_device(
    residual_in,
    conv_values,
    conv_gates,
    conv_kernel,
    conv_bias,
    chan_gain,
    chan_shift,
    out_weight,
    norm_gain,
    route_ids,
    route_weights,
    expert_gate,
    expert_up,
    expert_down,
):
    sp_count = lax.axis_size("sp")
    experts_all = expert_gate.shape[0] * sp_count
    choose_count, row_count = route_ids.shape[1], residual_in.shape[0]
    slot_cap = max(2, (2 * choose_count * row_count + experts_all - 1) // experts_all)
    slot_cap = (slot_cap + 15) // 16 * 16
    return run_layer(
        conv_values,
        conv_gates,
        conv_kernel,
        conv_bias[None, :],
        chan_gain[None, :],
        chan_shift[None, :],
        norm_gain[None, :],
        route_ids.T,
        route_weights.T,
        residual_in,
        out_weight,
        expert_gate,
        expert_up,
        expert_down,
        sp_count,
        slot_cap,
    )


def solution(mesh):
    placed = (
        P(("sp", "tp"), None),
        P("sp", "tp"),
        P("sp", "tp"),
        P(None, "tp"),
        P("tp"),
        P("tp"),
        P("tp"),
        P(),
        P(),
        P(("sp", "tp"), None),
        P(("sp", "tp"), None),
        P("sp", None, "tp"),
        P("sp", None, "tp"),
        P("sp", "tp", None),
    )
    return jax.shard_map(
        on_device, mesh=mesh, in_specs=placed, out_specs=P(("sp", "tp"), None), check_vma=False
    )
```

```python
import functools

import jax
import jax.numpy as jnp
from jax import lax
from jax.experimental import pallas as pl
from jax.experimental.pallas import tpu as pltpu
from jax.sharding import PartitionSpec as P

PLANES = 4
CHUNKS = 8
MESH = pl.DeviceIdType.MESH


def flipped(index, offset):
    result, bit = index, 1
    while bit <= offset:
        if offset & bit:
            result = result + bit * (1 - 2 * ((index // bit) % 2))
        bit *= 2
    return result


def layer_kernel(
    count, cap, values, gates, taps, bias, gain, shift, norm_gain, ids, scales,
    residual_in, mix_in, gate_in, up_in, down_in, out,
    dense, pick, rows, part, given, hidden, ret, zout, zin, gate_w, up_w, down_w,
    extended, mixed, tail, stats, swapped, acted, route, picks, weights, projected,
    disp_sent, disp_came, plane_sent, plane_came, pair_sent, pair_came, part_sent, part_came,
    back_sent, back_came, chain_sent, chain_came, loaded, mix_sent, mix_came,
):
    me, core = lax.axis_index("sp"), lax.axis_index("tp")
    other = 1 - core
    row_count, width = dense.shape[1], dense.shape[2]
    tok_count, chan = values.shape
    taps_count, groups = taps.shape[0], chan // 128
    pad = extended.shape[1] - tok_count
    after = zout.at[0]
    chips = count // PLANES
    half = chips * cap
    z = me // chips
    mid = ((z + 1) // 2) % 2
    low = z // 2
    sources = (z, z + 1 - 2 * (z % 2), 3 * (1 - low), 2 - low)
    flips = (0, 1, 3 - mid, 2 + mid)
    ways = (0, 1 - 2 * (z % 2), 1 - 2 * low, 1 - 2 * low)
    landings = (
        0,
        sources[1] + (PLANES - sources[1]) * (z % 2),
        sources[2],
        sources[3] + (PLANES - sources[3]) * low * (1 - z % 2),
    )
    inner = 1 - 2 * low
    is_mid, is_end = mid == 1, mid == 0
    crossed = (z, z + 1 - 2 * (z % 2), z + 2 - 4 * low, PLANES - 1 - z)
    aways = (0, 2 * (z % 2) - 1, 2 * low - 1, 2 * low - 1)
    has_left, has_right = z > 0, z < PLANES - 1
    wide = width // CHUNKS
    own = dense.at[z]

    def cols(number):
        return pl.ds(pl.multiple_of(number * wide, wide), wide)

    def pairs(number):
        return pl.ds(pl.multiple_of(number * 2 * wide, 2 * wide), 2 * wide)

    def every(number):
        return pl.ds(0, CHUNKS * wide) if number is None else cols(number)

    def along(way):
        return {"sp": me + way * chips}

    def dispatch(source, number, way, slot, block=None):
        block = dense.at[source] if block is None else block
        return pltpu.make_async_remote_copy(
            src_ref=block.at[:, cols(number)],
            dst_ref=dense.at[source, :, cols(number)],
            send_sem=disp_sent.at[slot],
            recv_sem=disp_came.at[source, number],
            device_id=along(way),
            device_id_type=MESH,
        )

    def plane_copy(turn, number, place, places=1):
        return pltpu.make_async_remote_copy(
            src_ref=pick.at[turn, pl.ds(place * cap, places * cap), cols(number)],
            dst_ref=rows.at[turn, pl.ds(place * cap, places * cap), cols(number)],
            send_sem=plane_sent.at[0],
            recv_sem=plane_came.at[turn, number],
            device_id={"sp": flipped(me, place)},
            device_id_type=MESH,
        )

    def pair_copy(turn, number):
        return pltpu.make_async_remote_copy(
            src_ref=rows.at[turn, pl.ds(0, half), every(number)],
            dst_ref=rows.at[turn, pl.ds(half, half), every(number)],
            send_sem=pair_sent.at[0],
            recv_sem=pair_came.at[turn],
            device_id={"tp": other},
            device_id_type=MESH,
        )

    def share_copy(turn, number):
        return pltpu.make_async_remote_copy(
            src_ref=part.at[turn, pl.ds(half, half), cols(number)],
            dst_ref=given.at[turn, :, cols(number)],
            send_sem=part_sent.at[0],
            recv_sem=part_came.at[turn, number],
            device_id={"tp": other},
            device_id_type=MESH,
        )

    def back_copy(turn, number, place, places=1):
        return pltpu.make_async_remote_copy(
            src_ref=part.at[turn, pl.ds(place * cap, places * cap), cols(number)],
            dst_ref=ret.at[turn, pl.ds(place * cap, places * cap), cols(number)],
            send_sem=back_sent.at[0],
            recv_sem=back_came.at[turn, number],
            device_id={"sp": flipped(me, place)},
            device_id_type=MESH,
        )

    def chain_copy(turn, number, landing=None):
        landing = landings[turn] if landing is None else landing
        return pltpu.make_async_remote_copy(
            src_ref=zout.at[turn, :, cols(number)],
            dst_ref=zin.at[landing, :, cols(number)],
            send_sem=chain_sent.at[0],
            recv_sem=chain_came.at[landing, number],
            device_id=along(ways[turn]),
            device_id_type=MESH,
        )

    loads = [
        pltpu.make_async_copy(source, target, loaded.at[number])
        for number, (source, target) in enumerate(
            (
                (gate_in.at[0], gate_w), (up_in.at[0], up_w), (down_in.at[0], down_w),
                (mix_in, down_w), (residual_in, after),
            )
        )
    ]
    early = loads[3:]
    loads = loads[:3]
    for load in early + loads[:2]:
        load.start()

    barrier = pltpu.get_barrier_semaphore()
    for place in range(1, chips):
        pl.semaphore_signal(
            barrier, inc=1, device_id={"sp": flipped(me, place)}, device_id_type=MESH
        )
    pl.semaphore_signal(barrier, inc=1, device_id={"tp": other}, device_id_type=MESH)

    for flip in range(1, PLANES):
        pl.semaphore_signal(
            barrier, inc=1, device_id={"sp": crossed[flip] * chips + me % chips}, device_id_type=MESH
        )

    def greet(step):
        pl.semaphore_signal(barrier, inc=1, device_id={"sp": me + step}, device_id_type=MESH)

    not_first, not_last = me > 0, me < count - 1
    pl.when(not_first)(lambda: greet(-1))
    pl.when(not_last)(lambda: greet(1))

    def gated(first_row, row_total, lanes):
        chosen = (pl.ds(first_row, row_total), lanes)
        return (
            values[chosen].astype(jnp.float32) * jax.nn.sigmoid(gates[chosen].astype(jnp.float32))
        ).astype(jnp.bfloat16)

    tail[0] = gated(tok_count - pad, pad, pl.ds(0, chan))
    pl.semaphore_wait(
        barrier,
        chips + PLANES - 1 + (me + count - 2) // (count - 1) + (2 * count - 3 - me) // (count - 1),
    )

    def mix_copy(source, target, number, device):
        return pltpu.make_async_remote_copy(
            src_ref=source,
            dst_ref=target,
            send_sem=mix_sent.at[number],
            recv_sem=mix_came.at[number],
            device_id=device,
            device_id_type=MESH,
        )

    halo = mix_copy(tail.at[0], tail.at[1], 0, {"sp": me + 1})
    moments = mix_copy(stats.at[0], stats.at[1], 1, {"tp": other})
    mine = pl.ds(pl.multiple_of(core * chan, chan), chan)
    exchange = mix_copy(swapped, acted.at[:, mine], 2, {"tp": other})
    routings = [
        mix_copy(
            route.at[0], route.at[flip], 2 + flip, {"sp": crossed[flip] * chips + me % chips}
        )
        for flip in range(1, PLANES)
    ]
    pl.when(not_last)(lambda: halo.start())

    experts_all = count
    expert_rows = lax.broadcasted_iota(jnp.int32, (experts_all, row_count), 0)
    named = [expert_rows == ids[choice : choice + 1, :] for choice in range(ids.shape[0])]
    onehot = sum(jnp.where(match, 1.0, 0.0) for match in named).astype(jnp.bfloat16)
    earlier = jnp.where(
        lax.broadcasted_iota(jnp.int32, (row_count, row_count), 0)
        < lax.broadcasted_iota(jnp.int32, (row_count, row_count), 1),
        1.0,
        0.0,
    ).astype(jnp.bfloat16)
    before = jnp.dot(onehot, earlier, preferred_element_type=jnp.float32)
    places = (
        (expert_rows // chips) * half
        + ((expert_rows % chips) ^ (me % chips)) * cap
    ).astype(jnp.float32) + before
    for choice, match in enumerate(named):
        route[0, choice : choice + 1, :] = jnp.sum(
            jnp.where(match, places, 0.0), 0, keepdims=True
        )
    lowest = ids.shape[0]
    route[0, lowest : 2 * lowest, :] = scales[...]
    for copy in routings:
        copy.start()

    for group in range(groups):
        extended[group, pl.ds(pad, tok_count), :] = gated(
            0, tok_count, pl.ds(group * 128, 128)
        ).astype(jnp.float32)

    block_rows = 64

    def convolve(number, carry):
        start = pl.multiple_of(number * block_rows, block_rows)
        total = jnp.zeros((block_rows, 128), jnp.float32)
        squares = total
        for group in range(groups):
            lanes = pl.ds(group * 128, 128)
            result = jnp.broadcast_to(bias[:, lanes], (block_rows, 128))
            for tap in range(taps_count):
                result = result + taps[tap : tap + 1, lanes] * (
                    extended[group, pl.ds(start + pad - taps_count + 1 + tap, block_rows), :]
                )
            mixed[group, pl.ds(start, block_rows), :] = result
            total = total + result
            squares = squares + result * result
        left = lax.broadcasted_iota(jnp.int32, (block_rows, 128), 1) < 64
        stats[0, pl.ds(start, block_rows), :] = jnp.where(
            left, jnp.sum(total, 1, keepdims=True), jnp.sum(squares, 1, keepdims=True)
        )
        return carry

    lax.fori_loop(1, tok_count // block_rows, convolve, 0)

    @pl.when(not_first)
    def _():
        halo.wait_recv()
        for group in range(groups):
            extended[group, pl.ds(0, pad), :] = tail[1, :, pl.ds(group * 128, 128)].astype(
                jnp.float32
            )

    @pl.when(me == 0)
    def _():
        extended[:, pl.ds(0, pad), :] = jnp.zeros((groups, pad, 128), jnp.float32)

    convolve(0, 0)
    moments.start()
    def clear(landing):
        zin[landing] = jnp.zeros((row_count, width), jnp.bfloat16)

    pl.when(jnp.logical_not(has_left))(lambda: clear(z))
    pl.when(jnp.logical_not(has_right))(lambda: clear(PLANES))
    moments.wait_recv()

    def activate(half_index, store):
        start = pl.multiple_of(half_index * row_count, row_count)
        both = stats[0, pl.ds(start, row_count), :] + stats[1, pl.ds(start, row_count), :]
        center = both[:, 0:1] / (2 * chan)
        scale = lax.rsqrt(both[:, 64:65] / (2 * chan) - center * center + 1e-06)
        for group in range(groups):
            lanes = pl.ds(group * 128, 128)
            normed = (mixed[group, pl.ds(start, row_count), :] - center) * scale * gain[
                :, lanes
            ] + shift[:, lanes]
            store(group, jax.nn.silu(normed).astype(jnp.bfloat16))

    def store_swapped(group, value):
        swapped[:, pl.ds(group * 128, 128)] = value

    def store_mine(group, value):
        acted[:, pl.ds(pl.multiple_of(core * chan + group * 128, 128), 128)] = value

    activate(other, store_swapped)
    exchange.start()
    activate(core, store_mine)
    for load in early:
        load.wait()
    ours = pl.ds(pl.multiple_of(core * chan, chan), chan)
    theirs = pl.ds(pl.multiple_of(other * chan, chan), chan)

    def half_project(number, carry):
        projected[:, pairs(number)] = after[:, pairs(number)].astype(jnp.float32) + jnp.dot(
            acted[:, ours], down_w[ours, pairs(number)], preferred_element_type=jnp.float32
        )
        return carry

    lax.fori_loop(0, CHUNKS // 2, half_project, 0)
    exchange.wait_recv()

    def project(number, carry):
        block = (
            projected[:, pairs(number)]
            + jnp.dot(
                acted[:, theirs], down_w[theirs, pairs(number)], preferred_element_type=jnp.float32
            )
        ).astype(jnp.bfloat16)
        after[:, pairs(number)] = block
        wider = block.astype(jnp.float32)
        return carry + jnp.sum(wider * wider, 1, keepdims=True)

    power = lax.fori_loop(0, CHUNKS // 2, project, jnp.zeros((row_count, 1), jnp.float32))
    loads[2].start()
    level = lax.rsqrt(power / width + 1e-06)

    def send_own(number, carry):
        own[:, cols(number)] = (
            after[:, cols(number)].astype(jnp.float32) * level * norm_gain[:, cols(number)]
        ).astype(jnp.bfloat16)
        pl.when(is_mid)(lambda: dispatch(z, number, -inner, 0).start())
        pl.when(is_end)(lambda: dispatch(z, number, inner, 1).start())
        return carry

    lax.fori_loop(0, CHUNKS, send_own, 0)

    def send_inner():
        def step(number, carry):
            dispatch(z, number, inner, 1).start()
            return carry

        pl.when(is_mid)(lambda: lax.fori_loop(0, CHUNKS, step, None))

    def place(flip):
        slots = (
            lax.broadcasted_iota(jnp.int32, (half, row_count), 0) + z * half
        ).astype(jnp.float32)
        matches = [slots == route[flip, choice : choice + 1, :] for choice in range(lowest)]
        picks[flip] = sum(jnp.where(match, 1.0, 0.0) for match in matches).astype(jnp.bfloat16)
        weighting = sum(
            jnp.where(match, route[flip, lowest + choice : lowest + choice + 1, :], 0.0)
            for choice, match in enumerate(matches)
        )
        coarse = weighting.astype(jnp.bfloat16)
        weights[flip, 0] = coarse
        weights[flip, 1] = (weighting - coarse.astype(jnp.float32)).astype(jnp.bfloat16)

    place(0)

    def select(turn, flip, block, number):
        chosen = jnp.dot(
            picks[flip], block[:, cols(number)], preferred_element_type=jnp.float32
        ).astype(jnp.bfloat16)
        rows[turn, pl.ds(0, cap), cols(number)] = chosen[:cap]
        pick[turn, :, cols(number)] = chosen
        for place in range(1, chips):
            plane_copy(turn, number, place).start()

    def arrive(turn, flip, number):
        source = crossed[flip]
        dispatch(source, number, 0, 0).wait_recv()
        pl.when(is_mid)(lambda: dispatch(source, number, aways[flip], 2).start())
        select(turn, flip, dense.at[source], number)

    def near(number):
        arrive(1, 1, number)

    def mid_next(number):
        pl.when(is_mid)(lambda: arrive(2, 2, number))

    def across(number):
        arrive(2 + mid, 3, number)

    def far(number):
        pl.when(is_end)(lambda: arrive(3, 2, number))

    def gather(turn):
        def step(number, carry):
            plane_copy(turn, number, 1, chips - 1).wait_recv()
            pair_copy(turn, number).start()
            return carry

        lax.fori_loop(0, CHUNKS, step, 0)
        if turn == 0:
            for load in loads:
                load.wait()

        pair_copy(turn, None).wait_recv()

    def first(turn, begin, end):
        narrow = min(256, gate_w.shape[1])

        def step(number, carry):
            columns = pl.ds(pl.multiple_of(number * narrow, narrow), narrow)
            gate = jnp.dot(rows[turn], gate_w[:, columns], preferred_element_type=jnp.float32)
            upper = jnp.dot(rows[turn], up_w[:, columns], preferred_element_type=jnp.float32)
            hidden[:, columns] = (jax.nn.silu(gate) * upper).astype(jnp.bfloat16)
            return carry

        blocks = gate_w.shape[1] // narrow
        lax.fori_loop(begin * blocks // CHUNKS, end * blocks // CHUNKS, step, 0)

    def second(turn, begin, end):
        def step(number, carry):
            part[turn, :, pairs(number)] = jnp.dot(
                hidden[...], down_w[:, pairs(number)], preferred_element_type=jnp.float32
            ).astype(jnp.bfloat16)
            share_copy(turn, 2 * number).start()
            share_copy(turn, 2 * number + 1).start()
            return carry

        lax.fori_loop(begin // 2, end // 2, step, 0)

    def third(turn, begin, end):
        def step(number, carry):
            share_copy(turn, number).wait_recv()
            total = (
                part[turn, pl.ds(0, half), cols(number)].astype(jnp.float32)
                + given[turn, :, cols(number)].astype(jnp.float32)
            ).astype(jnp.bfloat16)
            part[turn, pl.ds(0, half), cols(number)] = total
            ret[turn, pl.ds(0, cap), cols(number)] = total[:cap]
            for place in range(1, chips):
                back_copy(turn, number, place).start()
            return carry

        lax.fori_loop(begin, end, step, 0)

    def combined(turn, number):
        back_copy(turn, number, 1, chips - 1).wait_recv()
        block = ret[turn, :, cols(number)]
        across = (((0,), (0,)), ((), ()))
        return lax.dot_general(
            weights[flips[turn], 0], block, across, preferred_element_type=jnp.float32
        ) + lax.dot_general(
            weights[flips[turn], 1], block, across, preferred_element_type=jnp.float32
        )

    def end_chain(turn, number):
        @pl.when(is_end)
        def _():
            zout[turn, :, cols(number)] = combined(turn, number).astype(jnp.bfloat16)
            chain_copy(turn, number).start()

    def mid_link(turn, number):
        partial = combined(turn, number)
        chain_copy(turn, number, sources[turn]).wait_recv()
        zout[turn, :, cols(number)] = (
            partial + zin[sources[turn], :, cols(number)].astype(jnp.float32)
        ).astype(jnp.bfloat16)
        chain_copy(turn, number).start()

    def run(*steps):
        for step, *rest in steps:
            step(*rest)

    G, F, U, T, C = gather, first, second, third, end_chain
    A, M, B, E = near, mid_next, across, far

    def R(turn, number):
        pl.when(is_mid)(lambda: mid_link(turn, number))

    for number in range(CHUNKS):
        select(0, 0, own, number)
    for flip in range(1, PLANES):
        routings[flip - 1].wait_recv()
        place(flip)
    run((A, 0), (A, 1), (A, 2), (M, 0), (A, 3), (M, 1), (G, 0), (F, 0, 0, 8))
    run((A, 4), (M, 2), (A, 5), (M, 3), (U, 0, 0, 4), (A, 6), (M, 4), (U, 0, 4, 8), (A, 7))
    run((send_inner,), (M, 5), (M, 6), (M, 7), (G, 1), (F, 1, 0, 4), (B, 0), (B, 1), (B, 2))
    run((F, 1, 4, 8), (B, 3), (U, 1, 0, 4), (B, 4), (T, 1, 0, 2), (U, 1, 4, 8), (T, 1, 2, 3), (B, 5))
    run((T, 1, 3, 4), (B, 6), (T, 1, 4, 5), (C, 1, 0), (B, 7))
    run((T, 1, 5, 6), (C, 1, 1), (C, 1, 2), (E, 0), (T, 1, 6, 8), (C, 1, 3), (E, 1), (G, 2))
    run((F, 2, 0, 4), (C, 1, 4), (C, 1, 5), (E, 2), (E, 3), (F, 2, 4, 8), (U, 2, 0, 4), (C, 1, 6))
    run((E, 4), (T, 2, 0, 2), (U, 2, 4, 8), (C, 1, 7), (E, 5), (E, 6), (E, 7))
    run((T, 2, 2, 6), (C, 2, 0), (T, 2, 6, 8), (C, 2, 1), (C, 2, 2), (C, 2, 3), (G, 3), (F, 3, 0, 4))
    run((C, 2, 4), (C, 2, 5), (F, 3, 4, 8), (R, 2, 0), (U, 3, 0, 4))
    run((C, 2, 6), (T, 3, 0, 2), (R, 2, 1), (U, 3, 4, 8), (T, 3, 2, 4), (C, 2, 7), (T, 3, 4, 8))
    run((R, 2, 2), (T, 0, 0, 8))
    for number in range(CHUNKS):
        end_chain(3, number)

    @pl.when(is_mid)
    def _():
        for number in range(CHUNKS):
            if number > 2:
                mid_link(2, number)
                mid_link(1, number - 3)
        for number in range(CHUNKS):
            mid_link(3, number)
            if number < 3:
                mid_link(1, CHUNKS - 3 + number)

    def finish(number, carry):
        total = after[:, cols(number)].astype(jnp.float32) + combined(0, number)
        pl.when(has_left)(lambda: chain_copy(1, number, z).wait_recv())
        pl.when(has_right)(lambda: chain_copy(1, number, PLANES).wait_recv())
        out[:, cols(number)] = (
            total
            + zin[z, :, cols(number)].astype(jnp.float32)
            + zin[PLANES, :, cols(number)].astype(jnp.float32)
        ).astype(jnp.bfloat16)
        return carry

    lax.fori_loop(0, CHUNKS, finish, 0)

    def sent(block, semaphore):
        return pltpu.make_async_remote_copy(
            src_ref=block,
            dst_ref=block,
            send_sem=semaphore.at[0],
            recv_sem=semaphore.at[0],
            device_id={"tp": other},
            device_id_type=MESH,
        )

    pl.when(not_last)(lambda: halo.wait_send())
    moments.wait_send()
    exchange.wait_send()
    for copy in routings:
        copy.wait_send()
    pl.when(is_mid)(lambda: sent(own, disp_sent).wait_send())
    sent(own, disp_sent.at[pl.ds(1, 1)]).wait_send()
    pl.when(is_mid)(
        lambda: sent(dense.at[pl.ds(0, PLANES - 1)], disp_sent.at[pl.ds(2, 1)]).wait_send()
    )
    sent(rows.at[:, pl.ds(0, half)], pair_sent).wait_send()
    sent(given, part_sent).wait_send()
    sent(pick.at[:, pl.ds(0, half - cap)], plane_sent).wait_send()
    sent(ret.at[:, pl.ds(0, half - cap)], back_sent).wait_send()
    sent(zout.at[pl.ds(1, PLANES - 1)], chain_sent).wait_send()


def run_layer(
    values, gates, taps, bias, gain, shift, norm_gain, ids, scales,
    residual_in, out_weight, expert_gate, expert_up, expert_down, count, cap,
):
    row_count, width = residual_in.shape
    tok_count, chan = values.shape
    units = expert_gate.shape[2]
    chips = count // PLANES
    half = chips * cap
    pad = (taps.shape[0] + 14) // 16 * 16
    groups = chan // 128
    choose_count = ids.shape[0]
    dma = lambda *shape: pltpu.SemaphoreType.DMA(shape)
    vmem = pl.BlockSpec(memory_space=pltpu.VMEM)
    anywhere = pl.BlockSpec(memory_space=pl.ANY)
    held = jnp.bfloat16
    return pl.pallas_call(
        functools.partial(layer_kernel, count, cap),
        out_shape=jax.ShapeDtypeStruct((row_count, width), held),
        in_specs=[vmem] * 9 + [anywhere] * 5,
        out_specs=vmem,
        scratch_shapes=[
            pltpu.VMEM((PLANES, row_count, width), held),
            pltpu.VMEM((PLANES, half, width), held),
            pltpu.VMEM((PLANES, 2 * half, width), held),
            pltpu.VMEM((PLANES, 2 * half, width), held),
            pltpu.VMEM((PLANES, half, width), held),
            pltpu.VMEM((2 * half, units), held),
            pltpu.VMEM((PLANES, half, width), held),
            pltpu.VMEM((PLANES, row_count, width), held),
            pltpu.VMEM((PLANES + 1, row_count, width), held),
            pltpu.VMEM((width, units), held),
            pltpu.VMEM((width, units), held),
            pltpu.VMEM((units, width), held),
            pltpu.VMEM((groups, pad + tok_count, 128), jnp.float32),
            pltpu.VMEM((groups, tok_count, 128), jnp.float32),
            pltpu.VMEM((2, pad, chan), held),
            pltpu.VMEM((2, tok_count, 128), jnp.float32),
            pltpu.VMEM((row_count, chan), held),
            pltpu.VMEM((row_count, 2 * chan), held),
            pltpu.VMEM((PLANES, 2 * choose_count, row_count), jnp.float32),
            pltpu.VMEM((PLANES, half, row_count), held),
            pltpu.VMEM((PLANES, 2, half, row_count), held),
            pltpu.VMEM((row_count, width), jnp.float32),
            dma(3), dma(PLANES, CHUNKS),
            dma(1), dma(PLANES, CHUNKS),
            dma(1), dma(PLANES),
            dma(1), dma(PLANES, CHUNKS),
            dma(1), dma(PLANES, CHUNKS),
            dma(1), dma(PLANES + 1, CHUNKS),
            dma(5), dma(2 + PLANES), dma(2 + PLANES),
        ],
        compiler_params=pltpu.CompilerParams(
            collective_id=0, has_side_effects=True, vmem_limit_bytes=63 * 1024 * 1024
        ),
    )(
        values, gates, taps, bias, gain, shift, norm_gain, ids, scales,
        residual_in, out_weight, expert_gate, expert_up, expert_down,
    )


def on_device(
    residual_in,
    conv_values,
    conv_gates,
    conv_kernel,
    conv_bias,
    chan_gain,
    chan_shift,
    out_weight,
    norm_gain,
    route_ids,
    route_weights,
    expert_gate,
    expert_up,
    expert_down,
):
    sp_count = lax.axis_size("sp")
    experts_all = expert_gate.shape[0] * sp_count
    choose_count, row_count = route_ids.shape[1], residual_in.shape[0]
    slot_cap = max(2, (2 * choose_count * row_count + experts_all - 1) // experts_all)
    slot_cap = (slot_cap + 15) // 16 * 16
    return run_layer(
        conv_values,
        conv_gates,
        conv_kernel,
        conv_bias[None, :],
        chan_gain[None, :],
        chan_shift[None, :],
        norm_gain[None, :],
        route_ids.T,
        route_weights.T,
        residual_in,
        out_weight,
        expert_gate,
        expert_up,
        expert_down,
        sp_count,
        slot_cap,
    )


def solution(mesh):
    placed = (
        P(("sp", "tp"), None),
        P("sp", "tp"),
        P("sp", "tp"),
        P(None, "tp"),
        P("tp"),
        P("tp"),
        P("tp"),
        P(),
        P(),
        P(("sp", "tp"), None),
        P(("sp", "tp"), None),
        P("sp", None, "tp"),
        P("sp", None, "tp"),
        P("sp", "tp", None),
    )
    return jax.shard_map(
        on_device, mesh=mesh, in_specs=placed, out_specs=P(("sp", "tp"), None), check_vma=False
    )
```
